32 devices in a mesh: rep: 2 (over x), fs: 8 (over z, y), tp: 2 (over core).
Axes of the slice: x: 2, y: 2, z: 4, core: 2. Of those that a mesh axis runs over, the one named last changes fastest.
Arguments:
- hidden_in: bfloat16 [10240, 2048], P(('rep', 'fs'), 'tp'), may hold values from -6 to 6
- mix_gain: float32 [2048], replicated, may hold values from 0.1 to 1.9
- w_value: bfloat16 [2048, 1024], P('fs', 'tp'), may hold values from -0.125 to 0.125
- w_gate: bfloat16 [2048, 1024], P('fs', 'tp'), may hold values from -0.125 to 0.125
- conv_taps: float32 [31, 1024], P(None, 'tp'), may hold values from -5 to 5
- conv_bias: float32 [1024], P('tp'), may hold values from -3 to 3
- chan_gain: float32 [1024], P('tp'), may hold values from 0.1 to 1.9
- chan_bias: float32 [1024], P('tp'), may hold values from -3 to 3
- w_back: bfloat16 [1024, 2048], P('tp', 'fs'), may hold values from -0.1875 to 0.1875
- feed_gain: float32 [2048], replicated, may hold values from 0.1 to 1.9
- w_up: bfloat16 [2048, 8192], P(None, ('fs', 'tp')), may hold values from -0.125 to 0.125
- w_down: bfloat16 [8192, 2048], P(('fs', 'tp')), may hold values from -0.0625 to 0.0625
Outputs:
- layer_out: bfloat16 [10240, 2048], P(('rep', 'fs'), 'tp')
The draws below stay inside these ranges and needn't reach their ends.
All inputs are finite; a program needn't handle non-finite values.
Results may differ from the reference program's by a relative error of at most 0.015.
Values may be sent and summed in bfloat16 or wider, within the bound.
A program may use at most 128 MiB of HBM per device.

```python
import jax
import jax.numpy as jnp
from jax import lax

D = 2048
CH = 1024
FF = 8192
KW = 31
LEN = 128
TOKENS = 10240
N_FS = 8
N_TP = 2


def draw_conv_taps(key, part):
    entry_key, rough_key = jax.random.split(jax.random.fold_in(key, 11))
    channel_ramp = jnp.arange(CH, dtype=jnp.float32) / CH
    roughness = jax.random.uniform(rough_key, (KW, CH), jnp.float32, 0.5, 1.5)
    entries = jnp.clip(jax.random.normal(entry_key, (KW, CH), jnp.float32), -4.0, 4.0)
    growth = 3.0 ** channel_ramp
    return (entries * roughness * growth[None, :] * KW ** (-0.5)).astype(jnp.float32)


def shard_levels(own_key, dims, cuts, least, high):
    loudness, own = 1.0, jax.random.fold_in(own_key, 6)
    for dim, blocks in cuts:
        heights = jnp.exp(jax.random.uniform(jax.random.fold_in(own, dim), (blocks,), jnp.float32, least / len(cuts), high / len(cuts)))
        loudness = loudness * jnp.repeat(heights, dims[dim] // blocks).reshape([-1 if axis == dim else 1 for axis in range(len(dims))])
    return loudness


def gaussian(own_key, extent, deviation, most, cuts=(), kind=jnp.bfloat16):
    values = deviation * jax.random.normal(own_key, extent, jnp.float32)
    if cuts:
        values = values * shard_levels(own_key, extent, cuts, -0.22, 0.18)
    return jnp.clip(values, -most, most).astype(kind)


def setup_inputs(seed: int = 0) -> dict:
    key_of = jax.random.split(jax.random.key(seed), 13)
    hidden_in = gaussian(key_of[0], (TOKENS, D), 1.0, 6.0, ((0, 16), (1, 2)))
    mix_gain = jnp.clip(1.0 + 0.18 * jax.random.normal(key_of[1], (D,), jnp.float32), 0.1, 1.9)
    w_value = gaussian(key_of[2], (D, CH), D ** -0.5, 0.125, ((0, 8), (1, 2)))
    w_gate = gaussian(key_of[3], (D, CH), D ** -0.5, 0.125, ((0, 8), (1, 2)))
    conv_taps = draw_conv_taps(jax.random.fold_in(key_of[12], 71), 0)
    conv_bias = gaussian(key_of[5], (CH,), 0.5, 3.0, ((0, 2),), jnp.float32)
    chan_gain = jnp.clip(1.0 + 0.18 * jax.random.normal(key_of[6], (CH,), jnp.float32), 0.1, 1.9)
    chan_bias = gaussian(key_of[7], (CH,), 0.5, 3.0, ((0, 2),), jnp.float32)
    w_back = gaussian(key_of[8], (CH, D), CH ** -0.5, 0.1875, ((0, 2), (1, 8)))
    feed_gain = jnp.clip(1.0 + 0.18 * jax.random.normal(key_of[9], (D,), jnp.float32), 0.1, 1.9)
    w_up = gaussian(key_of[10], (D, FF), D ** -0.5, 0.125, ((1, 16),))
    w_down = gaussian(key_of[11], (FF, D), FF ** -0.5, 0.0625, ((0, 16),))
    return dict(hidden_in=hidden_in, mix_gain=mix_gain, w_value=w_value, w_gate=w_gate, conv_taps=conv_taps, conv_bias=conv_bias, chan_gain=chan_gain, chan_bias=chan_bias, w_back=w_back, feed_gain=feed_gain, w_up=w_up, w_down=w_down)


def rms_norm(stream, gain):
    values = stream.astype(jnp.float32)
    scaled = values * lax.rsqrt(lax.optimization_barrier(jnp.mean(values * values, axis=-1, keepdims=True)) + 1e-06)
    return (scaled * gain).astype(jnp.bfloat16)

def causal_filter(gated, conv_taps, conv_bias):
    channels = gated.shape[1]
    blocks = gated.reshape(gated.shape[0] // LEN, LEN, channels)
    padded = jnp.pad(blocks, ((0, 0), (KW - 1, 0), (0, 0)))
    result = jnp.zeros_like(blocks) + conv_bias
    for tap_index in range(KW):
        result = result + conv_taps[tap_index] * padded[:, tap_index:tap_index + LEN]
    return result.reshape(gated.shape)

def blocked_sum(left, right):
    inner = left.shape[1] // N_TP
    running = jnp.zeros((left.shape[0], right.shape[1]), jnp.float32)
    for block_index in range(N_TP):
        partial_value = jnp.dot(left[:, block_index * inner:(block_index + 1) * inner], right[block_index * inner:(block_index + 1) * inner], preferred_element_type=jnp.float32)
        running = running + partial_value.astype(jnp.bfloat16).astype(jnp.float32)
    return running

def strided_sum(left, right):
    rows = left.shape[0]
    width = right.shape[1]
    block = left.shape[1] // (N_FS * N_TP)
    left_blocks = left.reshape(rows, N_FS, N_TP, block)
    right_blocks = right.reshape(N_FS, N_TP, block, width)
    running = jnp.zeros((rows, width), jnp.float32)
    for block_index in range(N_TP):
        partial_value = jnp.dot(left_blocks[:, :, block_index].reshape(rows, N_FS * block), right_blocks[:, block_index].reshape(N_FS * block, width), preferred_element_type=jnp.float32)
        running = running + partial_value.astype(jnp.bfloat16).astype(jnp.float32)
    return running

def reference(hidden_in, mix_gain, w_value, w_gate, conv_taps, conv_bias, chan_gain, chan_bias, w_back, feed_gain, w_up, w_down):
    normed = rms_norm(hidden_in, mix_gain)
    value_proj = jnp.dot(normed, w_value, preferred_element_type=jnp.float32)
    gate_proj = jnp.dot(normed, w_gate, preferred_element_type=jnp.float32)
    gated = value_proj * jax.nn.sigmoid(gate_proj)
    filtered = causal_filter(gated, conv_taps, conv_bias)
    chan_mean = lax.optimization_barrier(jnp.mean(filtered, axis=1, keepdims=True))
    chan_var = lax.optimization_barrier(jnp.mean(filtered * filtered, axis=1, keepdims=True)) - chan_mean * chan_mean
    centred = (filtered - chan_mean) * lax.rsqrt(chan_var + 1e-05) * chan_gain + chan_bias
    mixer_act = jax.nn.silu(centred).astype(jnp.bfloat16)
    mixed = blocked_sum(mixer_act, w_back)
    second = (hidden_in.astype(jnp.float32) + mixed).astype(jnp.bfloat16)
    normed_feed = rms_norm(second, feed_gain)
    up_proj = jnp.dot(normed_feed, w_up, preferred_element_type=jnp.float32)
    hidden = jnp.square(jax.nn.relu(up_proj)).astype(jnp.bfloat16)
    feed = strided_sum(hidden, w_down)
    return (second.astype(jnp.float32) + feed).astype(jnp.bfloat16)
```

```python
import jax
import jax.numpy as jnp
from jax import lax
from jax.sharding import Mesh, PartitionSpec as P

from jax.experimental import pallas as pl
from jax.experimental.pallas import tpu as pltpu


KW = 31
LEN = 128


SWAP = [(0, 1), (1, 0)]


def swap(value, axis):
    return lax.ppermute(value, axis, SWAP)


def ordered(own, other, index, axis):
    first = jnp.where(index == 0, own, other)
    return jnp.concatenate([first, jnp.where(index == 0, other, own)], axis=axis)


def own_first(array, index, axis):
    half = array.shape[axis] // 2
    return jnp.concatenate(
        [
            lax.dynamic_slice_in_dim(array, index * half, half, axis),
            lax.dynamic_slice_in_dim(array, (1 - index) * half, half, axis),
        ],
        axis=axis,
    )


def rms_norm(stream, gain):
    values = stream.astype(jnp.float32)
    scaled = values * lax.rsqrt(jnp.mean(values * values, axis=-1, keepdims=True) + 1e-06)
    return (scaled * gain).astype(jnp.bfloat16)


def causal_filter(gated, conv_taps, conv_bias):
    channels = gated.shape[1]
    blocks = gated.reshape(gated.shape[0] // LEN, LEN, channels)
    padded = jnp.pad(blocks, ((0, 0), (KW - 1, 0), (0, 0)))
    result = jnp.zeros_like(blocks) + conv_bias
    for tap_index in range(KW):
        result = result + conv_taps[tap_index] * padded[:, tap_index : tap_index + LEN]
    return result.reshape(gated.shape)


def plane_slots(piece):
    half = piece.shape[0] // 2
    from_rep = swap(piece, "rep")
    from_fy = swap(piece, "fy")
    diag_low = swap(from_rep[:half], "fy")
    diag_high = swap(from_fy[half:], "rep")
    return [piece, from_rep, from_fy, jnp.concatenate([diag_low, diag_high], axis=0)]


def full_features(slot):
    return jnp.concatenate([slot, swap(slot, "tp")], axis=1)


def tp_reduced(left, right):
    width = right.shape[1] // 2
    sent = jnp.dot(left, right[:, width:], preferred_element_type=jnp.float32)
    kept = jnp.dot(left, right[:, :width], preferred_element_type=jnp.float32)
    return kept + swap(sent.astype(jnp.bfloat16), "tp").astype(jnp.float32)


def plane_reduced(compute):
    diag = compute(3)
    half = diag.shape[0] // 2
    via_rep = swap(diag[:half].astype(jnp.bfloat16), "rep").astype(jnp.float32)
    via_fy = swap(diag[half:].astype(jnp.bfloat16), "fy").astype(jnp.float32)
    for_rep = compute(1)
    for_rep = jnp.concatenate([for_rep[:half], for_rep[half:] + via_fy], axis=0)
    from_rep = swap(for_rep.astype(jnp.bfloat16), "rep")
    for_fy = compute(2)
    for_fy = jnp.concatenate([for_fy[:half] + via_rep, for_fy[half:]], axis=0)
    from_fy = swap(for_fy.astype(jnp.bfloat16), "fy")
    return compute(0) + from_rep.astype(jnp.float32) + from_fy.astype(jnp.float32)


def block(
    hidden_in,
    mix_gain,
    w_value,
    w_gate,
    conv_taps,
    conv_bias,
    chan_gain,
    chan_bias,
    w_back,
    feed_gain,
    w_up,
    w_down,
):
    rep, fy, tp = lax.axis_index("rep"), lax.axis_index("fy"), lax.axis_index("tp")
    n_fz = lax.axis_size("fz")
    n_rep, n_fy, n_tp = lax.axis_size("rep"), lax.axis_size("fy"), lax.axis_size("tp")
    parts = n_rep * n_fy
    mine, theirs = rep * n_fy + fy, rep * n_fy + 1 - fy
    rows, back_cols = w_value.shape[0], w_back.shape[1]
    own_ch = w_value.shape[1] // parts

    def columns(array, which):
        return lax.dynamic_slice_in_dim(array, which * own_ch, own_ch, array.ndim - 1)

    def front_pack(which):
        packed_out = lax.dynamic_slice_in_dim(w_back, which * own_ch, own_ch, 0)
        pieces = [packed_out]
        if back_cols > own_ch:
            pieces = [
                packed_out[:, at : at + own_ch] for at in range(0, back_cols, own_ch)
            ]
        elif back_cols < own_ch:
            pieces = [packed_out.reshape(-1, own_ch)]
        return jnp.concatenate([columns(w_value, which), columns(w_gate, which)] + pieces, axis=0)

    received = swap(front_pack(theirs), "fy")
    slots = plane_slots(hidden_in)
    pair = ordered(front_pack(mine)[None], received[None], fy, 0)
    front = lax.all_gather(pair, "fz", axis=0, tiled=True)
    blocks = n_fz * n_fy
    w_in = own_first(
        jnp.concatenate(
            [
                front[:, :rows].reshape(blocks * rows, own_ch),
                front[:, rows : 2 * rows].reshape(blocks * rows, own_ch),
            ],
            axis=1,
        ),
        tp,
        0,
    )
    if back_cols >= own_ch:
        whole_back = front[:, 2 * rows :].reshape(blocks * (back_cols // own_ch), own_ch, own_ch)
    else:
        whole_back = front[:, 2 * rows :].reshape(blocks, own_ch, back_cols)
    whole_back = own_first(
        whole_back.transpose(1, 0, 2).reshape(own_ch, blocks * back_cols), tp, 1
    )

    own_ff = w_up.shape[1] // n_rep
    up_part = own_first(lax.dynamic_slice_in_dim(w_up, rep * own_ff, own_ff, 1), tp, 0)
    down_part = own_first(lax.dynamic_slice_in_dim(w_down, rep * own_ff, own_ff, 0), tp, 1)
    up = lax.all_gather(up_part, "fz", axis=1, tiled=True)
    down = lax.all_gather(down_part, "fz", axis=0, tiled=True)

    taps, bias = columns(conv_taps, mine), columns(conv_bias, mine)
    gain, shift = columns(chan_gain, mine), columns(chan_bias, mine)

    tokens = hidden_in.shape[0]
    mix_rolled, feed_rolled = own_first(mix_gain, tp, 0), own_first(feed_gain, tp, 0)
    gated = []
    for slot in slots:
        normed = rms_norm(full_features(slot), mix_rolled)
        both = jnp.dot(normed, w_in, preferred_element_type=jnp.float32)
        gated.append(both[:, :own_ch] * jax.nn.sigmoid(both[:, own_ch:]))
    filtered = causal_filter(jnp.concatenate(gated, axis=0), taps, bias)
    stats = jnp.stack([jnp.sum(filtered, axis=1), jnp.sum(filtered * filtered, axis=1)])
    stats = stats.reshape(2, 4, tokens)
    stats = stats + swap(stats, "tp")
    other = swap(stats, "rep")
    stats = stats + jnp.stack([other[:, at] for at in (1, 0, 3, 2)], axis=1)
    other = swap(stats, "fy")
    stats = stats + jnp.stack([other[:, at] for at in (2, 3, 0, 1)], axis=1)
    stats = stats.reshape(2, 4 * tokens) / (own_ch * parts * n_tp)
    chan_mean = stats[0][:, None]
    chan_var = stats[1][:, None] - chan_mean * chan_mean
    centred = (filtered - chan_mean) * lax.rsqrt(chan_var + 1e-05) * gain + shift
    act = jax.nn.silu(centred).astype(jnp.bfloat16)

    def mixed_share(index):
        return tp_reduced(act[index * tokens : (index + 1) * tokens], whole_back)

    mixed = plane_reduced(mixed_share)
    second = (hidden_in.astype(jnp.float32) + mixed).astype(jnp.bfloat16)

    hidden = []
    for slot in plane_slots(second):
        normed = rms_norm(full_features(slot), feed_rolled)
        up_proj = jnp.dot(normed, up, preferred_element_type=jnp.float32)
        hidden.append(jnp.square(jax.nn.relu(up_proj)).astype(jnp.bfloat16))
    hidden = list(lax.optimization_barrier(tuple(hidden)))

    def feed_share(index):
        return tp_reduced(hidden[index], down)

    feed = plane_reduced(feed_share)
    return (second.astype(jnp.float32) + feed).astype(jnp.bfloat16)


MESH = pl.DeviceIdType.MESH
LINE = 4
STAGES = 4
SENDS = 160
RECEIVES = 100
LANES = 128
HALO = 32


def fused_kernel(
    hidden_hbm,
    mix_gain,
    value_hbm,
    gate_hbm,
    taps,
    bias,
    chan_gain,
    chan_bias,
    back_hbm,
    feed_gain,
    up_hbm,
    down_hbm,
    out,
    stream,
    feat,
    front,
    back,
    halo,
    filtered,
    act,
    stats,
    stats_in,
    mix_out,
    mix_in,
    kept,
    second,
    square,
    square_in,
    up,
    down,
    hidden,
    pair_out,
    pair_in,
    plane_out,
    diag_in,
    rep_in,
    fy_in,
    local_sem,
    send_sem,
    recv_sem,
):
    f32, bf16 = jnp.float32, jnp.bfloat16
    rep, z, fy, tp = (lax.axis_index(name) for name in ("rep", "fz", "fy", "tp"))
    zs = (z, z + 1 - 2 * lax.rem(z, 2), lax.rem(z + LINE // 2, LINE), LINE - 1 - z)
    middle = lax.rem(z, LINE - 1) != 0
    to_rep, to_fy, to_tp = {"rep": 1 - rep}, {"fy": 1 - fy}, {"tp": 1 - tp}
    tokens, half = second.shape
    rows, chans = value_hbm.shape
    cols = chans // 2
    back_cols = back_hbm.shape[1]
    own_ff = up_hbm.shape[1] // 2
    ff = up.shape[1]
    width = 2 * half
    sent, slots = [], {}
    own_lanes = pl.ds(pl.multiple_of(tp * half, half), half)

    barrier = pltpu.get_barrier_semaphore()
    partners = [to_rep, to_fy, to_tp] + [{"fz": zs[at]} for at in range(1, LINE)]
    for partner in partners:
        pl.semaphore_signal(barrier, inc=1, device_id=partner, device_id_type=MESH)
    pl.semaphore_wait(barrier, len(partners))

    def slot(key):
        if key not in slots:
            slots[key] = len(slots)
            assert len(slots) <= RECEIVES
        return recv_sem.at[slots[key]]

    def push(key, src, device, dst=None, when=None):
        place = send_sem.at[len(sent)]
        arrive = slot(key)

        def copy():
            return pltpu.make_async_remote_copy(
                src_ref=src,
                dst_ref=src if dst is None else dst,
                send_sem=place,
                recv_sem=arrive,
                device_id=device,
                device_id_type=MESH,
            )

        sent.append((copy, when))
        assert len(sent) <= SENDS
        if when is None:
            copy().start()
        else:
            pl.when(when)(lambda: copy().start())

    def recv(key, ref):
        pltpu.make_async_remote_copy(
            src_ref=ref,
            dst_ref=ref,
            send_sem=send_sem.at[0],
            recv_sem=slot(key),
            device_id=to_tp,
            device_id_type=MESH,
        ).wait_recv()

    def local(index, pairs):
        for src, dst in pairs:
            pltpu.make_async_copy(src, dst, local_sem.at[index]).start()

    def local_wait(index, ref):
        pltpu.make_async_copy(ref, ref, local_sem.at[index]).wait()

    def block(index, which, size):
        return pl.ds(pl.multiple_of((zs[index] * 2 + which) * size, size), size)

    def front_half(index, which, side):
        return front.at[side, :, block(index, which, rows), :]

    def front_block(index, which):
        return front.at[:, :, block(index, which, rows), :]

    back_side = pl.ds(pl.multiple_of(rep * (chans // 2), chans // 2), chans // 2)
    back_far = pl.ds(pl.multiple_of((1 - rep) * (chans // 2), chans // 2), chans // 2)

    def back_half(index, which, side):
        return back.at[side, block(index, which, back_cols)]

    def back_block(index, which):
        return back.at[:, block(index, which, back_cols)]

    def unit(index):
        return pl.ds(pl.multiple_of(zs[index] * own_ff, own_ff), own_ff)

    up_rows = width // 2

    def up_piece(part):
        return lambda index: up.at[part * up_rows : (part + 1) * up_rows, unit(index)]

    step = half // STAGES

    def down_piece(part):
        return lambda index: down.at[:, unit(index), part * step : (part + 1) * step]

    def line_send(key, piece):
        push((key, 2), piece(0), {"fz": zs[2]})
        push((key, 3), piece(0), {"fz": zs[3]}, when=middle)
        push((key, 1), piece(0), {"fz": zs[1]})

    def line_relay(key, piece):
        recv((key, 2), piece(2))
        push((key, 3), piece(2), {"fz": zs[1]}, when=middle)

    local(0, [(hidden_hbm, stream.at[:, own_lanes])])
    push("hid", hidden_hbm, to_tp, stream.at[:, own_lanes])
    mine = block(0, fy, rows)
    local(
        1,
        [
            (hbm.at[:, side * cols : (side + 1) * cols], front.at[side, kind, mine, :])
            for side in range(2)
            for kind, hbm in enumerate((value_hbm, gate_hbm))
        ],
    )
    local(2, [(back_hbm, back_block(0, fy))])
    ff_part = pl.ds(pl.multiple_of(rep * own_ff, own_ff), own_ff)
    local(3, [(up_hbm.at[:, ff_part], up.at[:, unit(0)])])
    local(
        4,
        [
            (down_hbm.at[ff_part, side * half : (side + 1) * half], down.at[side, unit(0), :])
            for side in range(2)
        ],
    )

    local_wait(1, front_block(0, fy))
    line_send("zf", lambda index: front_half(index, fy, rep))
    push(("yf", 0), front_block(0, fy), to_fy)
    local_wait(2, back_block(0, fy))
    line_send("zb", lambda index: back_half(index, fy, back_side))

    halo[:, :HALO, :] = jnp.zeros((halo.shape[0], HALO, halo.shape[2]), f32)
    local_wait(0, stream.at[:, own_lanes])
    recv("hid", stream.at[:, pl.ds(pl.multiple_of((1 - tp) * half, half), half)])

    def norm_rows(at, carry):
        place = pl.ds(pl.multiple_of(at * 32, 32), 32)
        values = stream[place, :].astype(f32)
        scale = lax.rsqrt(jnp.sum(values * values, axis=-1, keepdims=True) / width + 1e-06)
        feat[0, place, :] = (values * scale * mix_gain[...]).astype(bf16)
        return carry

    lax.fori_loop(0, tokens // 32, norm_rows, 0)

    def front_on(index):
        push(("yf", index), front_half(index, fy, rep), to_fy)
        push(("xf", 0, index), front_half(index, fy, rep), to_rep)

    def front_turn(index):
        recv(("yf", index), front_half(index, 1 - fy, rep))
        push(("xf", 1, index), front_half(index, 1 - fy, rep), to_rep)

    def back_on(index):
        push(("yb", index), back_half(index, fy, back_side), to_fy)
        push(("xb", 0, index), back_half(index, fy, back_side), to_rep)

    def back_turn(index):
        recv(("yb", index), back_half(index, 1 - fy, back_side))
        push(("xb", 1, index), back_half(index, 1 - fy, back_side), to_rep)

    recv(("zf", 1), front_half(1, fy, rep))
    front_on(1)
    line_relay("zf", lambda index: front_half(index, fy, rep))
    front_on(2)
    front_turn(1)
    recv(("zf", 3), front_half(3, fy, rep))
    front_on(3)
    front_turn(2)
    push(("yb", 0), back_block(0, fy), to_fy)
    recv(("zb", 1), back_half(1, fy, back_side))
    line_relay("zb", lambda index: back_half(index, fy, back_side))
    local_wait(3, up.at[:, unit(0)])
    line_send(("up", 0), up_piece(0))
    front_turn(3)
    back_on(1)
    back_on(2)
    recv(("zb", 3), back_half(3, fy, back_side))
    back_on(3)
    line_send(("up", 1), up_piece(1))

    recv(("yf", 0), front_block(0, 1 - fy))
    for index in range(1, LINE):
        recv(("xf", 0, index), front_half(index, fy, 1 - rep))
        recv(("xf", 1, index), front_half(index, 1 - fy, 1 - rep))

    sequences = tokens // LEN
    for side in range(2):
        value = jnp.dot(feat[0], front[side, 0], preferred_element_type=f32)
        gate = jnp.dot(feat[0], front[side, 1], preferred_element_type=f32)
        gated = value * jax.nn.sigmoid(gate)
        halo[:, HALO:, side * cols : (side + 1) * cols] = gated.reshape(sequences, LEN, cols)

    for index in range(1, LINE):
        back_turn(index)

    def filter_sequence(at, carry):
        place = pl.ds(pl.multiple_of(at * LEN, LEN), LEN)
        total = jnp.zeros((LEN, LANES), f32)
        squares = jnp.zeros((LEN, LANES), f32)
        for lane in range(chans // LANES):
            lanes = slice(lane * LANES, (lane + 1) * LANES)
            result = jnp.zeros((LEN, LANES), f32) + bias[:, lanes]
            for tap in range(KW):
                start = HALO - KW + 1 + tap
                result = result + taps[tap : tap + 1, lanes] * halo[at, start : start + LEN, lanes]
            filtered[place, lanes] = result
            total = total + result
            squares = squares + result * result
        stats[0, place, :] = total
        stats[1, place, :] = squares
        return carry

    lax.fori_loop(0, sequences, filter_sequence, 0)
    push("stats", stats, to_tp, stats_in)
    line_relay(("up", 0), up_piece(0))
    recv("stats", stats_in)

    def act_rows(at, carry):
        place = pl.ds(pl.multiple_of(at * 32, 32), 32)
        count = 2 * chans
        mean = jnp.sum(stats[0, place, :] + stats_in[0, place, :], axis=-1, keepdims=True) / count
        second_moment = (
            jnp.sum(stats[1, place, :] + stats_in[1, place, :], axis=-1, keepdims=True) / count
        )
        scale = lax.rsqrt(second_moment - mean * mean + 1e-05)
        centred = (filtered[place, :] - mean) * scale * chan_gain[...] + chan_bias[...]
        act[place, :] = (centred * jax.nn.sigmoid(centred)).astype(bf16)
        return carry

    lax.fori_loop(0, tokens // 32, act_rows, 0)

    recv(("yb", 0), back_block(0, 1 - fy))
    for index in range(1, LINE):
        recv(("xb", 0, index), back_half(index, fy, back_far))
        recv(("xb", 1, index), back_half(index, 1 - fy, back_far))

    def back_lanes(side, part):
        return pl.ds(pl.multiple_of(side * half + part * step, step), step)

    for part in range(STAGES):
        lanes = slice(part * step, (part + 1) * step)
        product = jnp.dot(act[...], back[:, back_lanes(1 - tp, part)], preferred_element_type=f32)
        mix_out[:, lanes] = product.astype(bf16)
    push("mix", mix_out, to_tp, mix_in)
    for part in range(STAGES):
        kept[part] = jnp.dot(act[...], back[:, back_lanes(tp, part)], preferred_element_type=f32)
    recv("mix", mix_in)

    def second_rows(at, carry):
        place = pl.ds(pl.multiple_of(at * 32, 32), 32)
        squares = jnp.zeros((32, LANES), f32)
        for part in range(STAGES):
            lanes = slice(part * step, (part + 1) * step)
            source = pl.ds(pl.multiple_of(tp * half + part * step, step), step)
            mixed = kept[part, place, :] + mix_in[place, lanes].astype(f32)
            value = (stream[place, source].astype(f32) + mixed).astype(bf16)
            second[place, lanes] = value
            value = value.astype(f32)
            value = value * value
            for lane in range(step // LANES):
                squares = squares + value[:, lane * LANES : (lane + 1) * LANES]
        square[place, :] = squares
        return carry

    lax.fori_loop(0, tokens // 32, second_rows, 0)
    push("square", square, to_tp, square_in)
    local_wait(4, down.at[:, unit(0), :])
    line_send(("down", 0), down_piece(0))
    recv("square", square_in)

    def feed_rows(at, carry):
        place = pl.ds(pl.multiple_of(at * 32, 32), 32)
        mean = jnp.sum(square[place, :] + square_in[place, :], axis=-1, keepdims=True) / width
        scale = lax.rsqrt(mean + 1e-06)
        values = second[place, :].astype(f32) * scale * feed_gain[:, own_lanes]
        feat[0, place, own_lanes] = values.astype(bf16)
        return carry

    part_rows = tokens // 2

    def feat_part(index, part, lanes):
        return feat.at[index, part * part_rows : (part + 1) * part_rows, lanes]

    other_lanes = pl.ds(pl.multiple_of((1 - tp) * half, half), half)

    def share(index, part):
        push(("pair", index, part), feat_part(index, part, own_lanes), to_tp)

    def shared(index):
        for part in range(2):
            recv(("pair", index, part), feat_part(index, part, other_lanes))

    for part in range(2):
        lax.fori_loop(part * part_rows // 32, (part + 1) * part_rows // 32, feed_rows, 0)
        push(("rep", part), feat_part(0, part, own_lanes), to_rep, feat_part(1, part, own_lanes))
        push(("fy", part), feat_part(0, part, own_lanes), to_fy, feat_part(2, part, own_lanes))
        share(0, part)

    def up_slot(index):
        shared(index)
        for part in range(ff // step):
            lanes = slice(part * step, (part + 1) * step)
            product = jnp.dot(feat[index], up[:, lanes], preferred_element_type=f32)
            hidden[index, :, lanes] = jnp.square(jnp.maximum(product, 0.0)).astype(bf16)

    recv(("rep", 0), feat_part(1, 0, own_lanes))
    push(("diag", 0), feat_part(1, 0, own_lanes), to_fy, feat_part(3, 0, own_lanes))
    share(1, 0)
    recv(("fy", 0), feat_part(2, 0, own_lanes))
    share(2, 0)
    line_relay(("up", 1), up_piece(1))
    line_send(("down", 1), down_piece(1))
    recv(("rep", 1), feat_part(1, 1, own_lanes))
    share(1, 1)
    recv(("fy", 1), feat_part(2, 1, own_lanes))
    push(("diag", 1), feat_part(2, 1, own_lanes), to_rep, feat_part(3, 1, own_lanes))
    share(2, 1)
    for part in range(2):
        for index in (1, 3):
            recv((("up", part), index), up_piece(part)(index))
    up_slot(0)
    up_slot(1)
    recv(("diag", 0), feat_part(3, 0, own_lanes))
    share(3, 0)
    line_relay(("down", 0), down_piece(0))
    up_slot(2)
    recv(("diag", 1), feat_part(3, 1, own_lanes))
    share(3, 1)
    up_slot(3)

    def products(stage, index):
        lanes = slice(stage * step, (stage + 1) * step)
        product = jnp.dot(hidden[index], down[1 - tp, :, lanes], preferred_element_type=f32)
        pair_out[index, :, lanes] = product.astype(bf16)
        push(
            ("sum", index, stage),
            pair_out.at[index, :, lanes],
            to_tp,
            pair_in.at[index, :, lanes],
        )
        kept[index] = jnp.dot(hidden[index], down[tp, :, lanes], preferred_element_type=f32)

    def paired(stage, index, first, last):
        lanes = slice(stage * step, (stage + 1) * step)
        return kept[index, first:last, :] + pair_in[index, first:last, lanes].astype(f32)

    for stage in range(STAGES):
        lanes = slice(stage * step, (stage + 1) * step)
        piece = down_piece(stage)
        if stage + 2 < STAGES:
            line_send(("down", stage + 2), down_piece(stage + 2))
        for index in (1, 3):
            recv((("down", stage), index), piece(index))
        whole = slice(stage * step, (stage + 1) * step)
        products(stage, 3)
        products(stage, 1)
        recv(("sum", 3, stage), pair_in.at[3, :, whole])
        plane_out[2, :, lanes] = paired(stage, 3, 0, tokens).astype(bf16)
        push(
            ("far", 0, stage),
            plane_out.at[2, :part_rows, whole],
            to_rep,
            diag_in.at[0, :, whole],
        )
        push(
            ("far", 1, stage),
            plane_out.at[2, part_rows:, whole],
            to_fy,
            diag_in.at[1, :, whole],
        )
        products(stage, 2)
        products(stage, 0)
        recv(("sum", 1, stage), pair_in.at[1, :, whole])
        plane_out[0, :part_rows, lanes] = paired(stage, 1, 0, part_rows).astype(bf16)
        recv(("far", 1, stage), diag_in.at[1, :, whole])
        plane_out[0, part_rows:, lanes] = (
            paired(stage, 1, part_rows, tokens) + diag_in[1, :, lanes].astype(f32)
        ).astype(bf16)
        push(("near", 0, stage), plane_out.at[0, :, whole], to_rep, rep_in.at[:, whole])
        recv(("sum", 2, stage), pair_in.at[2, :, whole])
        plane_out[1, part_rows:, lanes] = paired(stage, 2, part_rows, tokens).astype(bf16)
        recv(("far", 0, stage), diag_in.at[0, :, whole])
        plane_out[1, :part_rows, lanes] = (
            paired(stage, 2, 0, part_rows) + diag_in[0, :, lanes].astype(f32)
        ).astype(bf16)
        push(("near", 1, stage), plane_out.at[1, :, whole], to_fy, fy_in.at[:, whole])
        recv(("sum", 0, stage), pair_in.at[0, :, whole])
        if stage + 1 < STAGES:
            line_relay(("down", stage + 1), down_piece(stage + 1))
        recv(("near", 0, stage), rep_in.at[:, whole])
        recv(("near", 1, stage), fy_in.at[:, whole])
        feed = paired(stage, 0, 0, tokens)
        feed = feed + rep_in[:, lanes].astype(f32) + fy_in[:, lanes].astype(f32)
        out[:, lanes] = (second[:, lanes].astype(f32) + feed).astype(bf16)

    for copy, when in sent:
        if when is None:
            copy().wait_send()
        else:
            pl.when(when)(lambda copy=copy: copy().wait_send())


def fused(*arrays):
    hidden_in, mix_gain, w_value, w_gate, taps, bias, gain, shift, w_back, feed_gain, w_up, w_down = arrays
    tokens, half = hidden_in.shape
    _, chans = w_value.shape
    width, ff = 2 * half, w_up.shape[1] // 2 * LINE
    bf16, f32 = jnp.bfloat16, jnp.float32
    vmem, hbm = pl.BlockSpec(memory_space=pltpu.VMEM), pl.BlockSpec(memory_space=pltpu.HBM)
    step = half // STAGES
    scratch = [
        ((tokens, width), bf16),
        ((4, tokens, width), bf16),
        ((2, 2, width, chans // 2), bf16),
        ((chans, width), bf16),
        ((tokens // LEN, HALO + LEN, chans), f32),
        ((tokens, chans), f32),
        ((tokens, chans), bf16),
        ((2, tokens, LANES), f32),
        ((2, tokens, LANES), f32),
        ((tokens, half), bf16),
        ((tokens, half), bf16),
        ((STAGES, tokens, step), f32),
        ((tokens, half), bf16),
        ((tokens, LANES), f32),
        ((tokens, LANES), f32),
        ((width, ff), bf16),
        ((2, ff, half), bf16),
        ((4, tokens, ff), bf16),
        ((4, tokens, half), bf16),
        ((4, tokens, half), bf16),
        ((3, tokens, half), bf16),
        ((2, tokens // 2, half), bf16),
        ((tokens, half), bf16),
        ((tokens, half), bf16),
    ]
    return pl.pallas_call(
        fused_kernel,
        out_shape=jax.ShapeDtypeStruct((tokens, half), bf16),
        in_specs=[hbm, vmem, hbm, hbm, vmem, vmem, vmem, vmem, hbm, vmem, hbm, hbm],
        out_specs=vmem,
        scratch_shapes=[pltpu.VMEM(shape, kind) for shape, kind in scratch]
        + [
            pltpu.SemaphoreType.DMA((5,)),
            pltpu.SemaphoreType.DMA((SENDS,)),
            pltpu.SemaphoreType.DMA((RECEIVES,)),
        ],
        compiler_params=pltpu.CompilerParams(
            collective_id=0, has_side_effects=True, vmem_limit_bytes=67043328
        ),
    )(
        hidden_in,
        mix_gain[None],
        w_value,
        w_gate,
        taps,
        bias[None],
        gain[None],
        shift[None],
        w_back,
        feed_gain[None],
        w_up,
        w_down,
    )


def fits(mesh):
    return mesh.shape["rep"] == 2 and mesh.shape["fs"] == 2 * LINE and mesh.shape["tp"] == 2


def solution(mesh):
    n_rep, n_fs, n_tp = mesh.shape["rep"], mesh.shape["fs"], mesh.shape["tp"]
    split = Mesh(mesh.devices.reshape(n_rep, n_fs // 2, 2, n_tp), ("rep", "fz", "fy", "tp"))
    fs = ("fz", "fy")
    rows = P(("rep", "fz", "fy"), "tp")
    placed = (
        rows,
        P(),
        P(fs, "tp"),
        P(fs, "tp"),
        P(None, "tp"),
        P("tp"),
        P("tp"),
        P("tp"),
        P("tp", fs),
        P(),
        P(None, ("fz", "fy", "tp")),
        P(("fz", "fy", "tp"), None),
    )
    if fits(mesh):
        return jax.shard_map(fused, mesh=split, in_specs=placed, out_specs=rows, check_vma=False)
    return jax.shard_map(block, mesh=split, in_specs=placed, out_specs=rows, check_vma=False)
```

```python
import jax
import jax.numpy as jnp
from jax import lax
from jax.sharding import Mesh, PartitionSpec as P

from jax.experimental import pallas as pl
from jax.experimental.pallas import tpu as pltpu


KW = 31
LEN = 128


SWAP = [(0, 1), (1, 0)]


def swap(value, axis):
    return lax.ppermute(value, axis, SWAP)


def ordered(own, other, index, axis):
    first = jnp.where(index == 0, own, other)
    return jnp.concatenate([first, jnp.where(index == 0, other, own)], axis=axis)


def own_first(array, index, axis):
    half = array.shape[axis] // 2
    return jnp.concatenate(
        [
            lax.dynamic_slice_in_dim(array, index * half, half, axis),
            lax.dynamic_slice_in_dim(array, (1 - index) * half, half, axis),
        ],
        axis=axis,
    )


def rms_norm(stream, gain):
    values = stream.astype(jnp.float32)
    scaled = values * lax.rsqrt(jnp.mean(values * values, axis=-1, keepdims=True) + 1e-06)
    return (scaled * gain).astype(jnp.bfloat16)


def causal_filter(gated, conv_taps, conv_bias):
    channels = gated.shape[1]
    blocks = gated.reshape(gated.shape[0] // LEN, LEN, channels)
    padded = jnp.pad(blocks, ((0, 0), (KW - 1, 0), (0, 0)))
    result = jnp.zeros_like(blocks) + conv_bias
    for tap_index in range(KW):
        result = result + conv_taps[tap_index] * padded[:, tap_index : tap_index + LEN]
    return result.reshape(gated.shape)


def plane_slots(piece):
    half = piece.shape[0] // 2
    from_rep = swap(piece, "rep")
    from_fy = swap(piece, "fy")
    diag_low = swap(from_rep[:half], "fy")
    diag_high = swap(from_fy[half:], "rep")
    return [piece, from_rep, from_fy, jnp.concatenate([diag_low, diag_high], axis=0)]


def full_features(slot):
    return jnp.concatenate([slot, swap(slot, "tp")], axis=1)


def tp_reduced(left, right):
    width = right.shape[1] // 2
    sent = jnp.dot(left, right[:, width:], preferred_element_type=jnp.float32)
    kept = jnp.dot(left, right[:, :width], preferred_element_type=jnp.float32)
    return kept + swap(sent.astype(jnp.bfloat16), "tp").astype(jnp.float32)


def plane_reduced(compute):
    diag = compute(3)
    half = diag.shape[0] // 2
    via_rep = swap(diag[:half].astype(jnp.bfloat16), "rep").astype(jnp.float32)
    via_fy = swap(diag[half:].astype(jnp.bfloat16), "fy").astype(jnp.float32)
    for_rep = compute(1)
    for_rep = jnp.concatenate([for_rep[:half], for_rep[half:] + via_fy], axis=0)
    from_rep = swap(for_rep.astype(jnp.bfloat16), "rep")
    for_fy = compute(2)
    for_fy = jnp.concatenate([for_fy[:half] + via_rep, for_fy[half:]], axis=0)
    from_fy = swap(for_fy.astype(jnp.bfloat16), "fy")
    return compute(0) + from_rep.astype(jnp.float32) + from_fy.astype(jnp.float32)


def block(
    hidden_in,
    mix_gain,
    w_value,
    w_gate,
    conv_taps,
    conv_bias,
    chan_gain,
    chan_bias,
    w_back,
    feed_gain,
    w_up,
    w_down,
):
    rep, fy, tp = lax.axis_index("rep"), lax.axis_index("fy"), lax.axis_index("tp")
    n_fz = lax.axis_size("fz")
    n_rep, n_fy, n_tp = lax.axis_size("rep"), lax.axis_size("fy"), lax.axis_size("tp")
    parts = n_rep * n_fy
    mine, theirs = rep * n_fy + fy, rep * n_fy + 1 - fy
    rows, back_cols = w_value.shape[0], w_back.shape[1]
    own_ch = w_value.shape[1] // parts

    def columns(array, which):
        return lax.dynamic_slice_in_dim(array, which * own_ch, own_ch, array.ndim - 1)

    def front_pack(which):
        packed_out = lax.dynamic_slice_in_dim(w_back, which * own_ch, own_ch, 0)
        pieces = [packed_out]
        if back_cols > own_ch:
            pieces = [
                packed_out[:, at : at + own_ch] for at in range(0, back_cols, own_ch)
            ]
        elif back_cols < own_ch:
            pieces = [packed_out.reshape(-1, own_ch)]
        return jnp.concatenate([columns(w_value, which), columns(w_gate, which)] + pieces, axis=0)

    received = swap(front_pack(theirs), "fy")
    slots = plane_slots(hidden_in)
    pair = ordered(front_pack(mine)[None], received[None], fy, 0)
    front = lax.all_gather(pair, "fz", axis=0, tiled=True)
    blocks = n_fz * n_fy
    w_in = own_first(
        jnp.concatenate(
            [
                front[:, :rows].reshape(blocks * rows, own_ch),
                front[:, rows : 2 * rows].reshape(blocks * rows, own_ch),
            ],
            axis=1,
        ),
        tp,
        0,
    )
    if back_cols >= own_ch:
        whole_back = front[:, 2 * rows :].reshape(blocks * (back_cols // own_ch), own_ch, own_ch)
    else:
        whole_back = front[:, 2 * rows :].reshape(blocks, own_ch, back_cols)
    whole_back = own_first(
        whole_back.transpose(1, 0, 2).reshape(own_ch, blocks * back_cols), tp, 1
    )

    own_ff = w_up.shape[1] // n_rep
    up_part = own_first(lax.dynamic_slice_in_dim(w_up, rep * own_ff, own_ff, 1), tp, 0)
    down_part = own_first(lax.dynamic_slice_in_dim(w_down, rep * own_ff, own_ff, 0), tp, 1)
    up = lax.all_gather(up_part, "fz", axis=1, tiled=True)
    down = lax.all_gather(down_part, "fz", axis=0, tiled=True)

    taps, bias = columns(conv_taps, mine), columns(conv_bias, mine)
    gain, shift = columns(chan_gain, mine), columns(chan_bias, mine)

    tokens = hidden_in.shape[0]
    mix_rolled, feed_rolled = own_first(mix_gain, tp, 0), own_first(feed_gain, tp, 0)
    gated = []
    for slot in slots:
        normed = rms_norm(full_features(slot), mix_rolled)
        both = jnp.dot(normed, w_in, preferred_element_type=jnp.float32)
        gated.append(both[:, :own_ch] * jax.nn.sigmoid(both[:, own_ch:]))
    filtered = causal_filter(jnp.concatenate(gated, axis=0), taps, bias)
    stats = jnp.stack([jnp.sum(filtered, axis=1), jnp.sum(filtered * filtered, axis=1)])
    stats = stats.reshape(2, 4, tokens)
    stats = stats + swap(stats, "tp")
    other = swap(stats, "rep")
    stats = stats + jnp.stack([other[:, at] for at in (1, 0, 3, 2)], axis=1)
    other = swap(stats, "fy")
    stats = stats + jnp.stack([other[:, at] for at in (2, 3, 0, 1)], axis=1)
    stats = stats.reshape(2, 4 * tokens) / (own_ch * parts * n_tp)
    chan_mean = stats[0][:, None]
    chan_var = stats[1][:, None] - chan_mean * chan_mean
    centred = (filtered - chan_mean) * lax.rsqrt(chan_var + 1e-05) * gain + shift
    act = jax.nn.silu(centred).astype(jnp.bfloat16)

    def mixed_share(index):
        return tp_reduced(act[index * tokens : (index + 1) * tokens], whole_back)

    mixed = plane_reduced(mixed_share)
    second = (hidden_in.astype(jnp.float32) + mixed).astype(jnp.bfloat16)

    hidden = []
    for slot in plane_slots(second):
        normed = rms_norm(full_features(slot), feed_rolled)
        up_proj = jnp.dot(normed, up, preferred_element_type=jnp.float32)
        hidden.append(jnp.square(jax.nn.relu(up_proj)).astype(jnp.bfloat16))
    hidden = list(lax.optimization_barrier(tuple(hidden)))

    def feed_share(index):
        return tp_reduced(hidden[index], down)

    feed = plane_reduced(feed_share)
    return (second.astype(jnp.float32) + feed).astype(jnp.bfloat16)


MESH = pl.DeviceIdType.MESH
LINE = 4
STAGES = 4
SENDS = 200
RECEIVES = 140
LANES = 128
HALO = 32


def fused_kernel(
    hidden_hbm,
    mix_gain,
    value_hbm,
    gate_hbm,
    taps,
    bias,
    chan_gain,
    chan_bias,
    back_hbm,
    feed_gain,
    up_hbm,
    down_hbm,
    out,
    stream,
    feat,
    front,
    back,
    halo,
    filtered,
    act,
    stats,
    stats_in,
    mix_out,
    mix_in,
    kept,
    second,
    square,
    square_in,
    up,
    down,
    hidden,
    pair_out,
    pair_in,
    plane_out,
    diag_in,
    rep_in,
    fy_in,
    local_sem,
    send_sem,
    recv_sem,
    pair_sem,
):
    f32, bf16 = jnp.float32, jnp.bfloat16
    rep, z, fy, tp = (lax.axis_index(name) for name in ("rep", "fz", "fy", "tp"))
    low = z // (LINE // 2)
    near, far, across = z + 1 - 2 * lax.rem(z, 2), lax.rem(z + LINE // 2, LINE), LINE - 1 - z
    zs = (z, near, LINE // 2 - low, (LINE - 1) * (1 - low))
    middle = lax.rem(z, LINE - 1) != 0
    ends = lax.rem(z, LINE - 1) == 0
    to_rep, to_fy, to_tp = {"rep": 1 - rep}, {"fy": 1 - fy}, {"tp": 1 - tp}
    to_line = {"fz": near}
    tokens, half = second.shape
    rows, chans = value_hbm.shape
    cols = chans // 2
    back_cols = back_hbm.shape[1]
    own_ff = up_hbm.shape[1] // 2
    width = 2 * half
    sent, slots, result = [], {}, mix_in
    own_lanes = pl.ds(pl.multiple_of(tp * half, half), half)

    barrier = pltpu.get_barrier_semaphore()
    partners = [to_rep, to_fy, to_tp] + [{"fz": at} for at in (near, far, across)]
    for partner in partners:
        pl.semaphore_signal(barrier, inc=1, device_id=partner, device_id_type=MESH)
    pl.semaphore_wait(barrier, len(partners))

    def slot(key):
        if key not in slots:
            slots[key] = len(slots)
            assert len(slots) <= RECEIVES
        return recv_sem.at[slots[key]]

    def push(key, src, device, dst=None, when=None):
        place = send_sem.at[len(sent)]
        arrive = slot(key)

        def copy():
            return pltpu.make_async_remote_copy(
                src_ref=src,
                dst_ref=src if dst is None else dst,
                send_sem=place,
                recv_sem=arrive,
                device_id=device,
                device_id_type=MESH,
            )

        sent.append((copy, when))
        assert len(sent) <= SENDS
        if when is None:
            copy().start()
        else:
            pl.when(when)(lambda: copy().start())

    def recv(key, ref, when=None):
        arrive = slot(key)

        def wait():
            pltpu.make_async_remote_copy(
                src_ref=ref,
                dst_ref=ref,
                send_sem=send_sem.at[0],
                recv_sem=arrive,
                device_id=to_tp,
                device_id_type=MESH,
            ).wait_recv()

        if when is None:
            wait()
        else:
            pl.when(when)(wait)

    def local(index, pairs):
        for src, dst in pairs:
            pltpu.make_async_copy(src, dst, local_sem.at[index]).start()

    def local_wait(index, ref):
        pltpu.make_async_copy(ref, ref, local_sem.at[index]).wait()

    def block(index, which, size):
        return pl.ds(pl.multiple_of((zs[index] * 2 + which) * size, size), size)

    def front_half(index, which, side):
        return front.at[side, :, block(index, which, rows), :]

    def front_block(index, which):
        return front.at[:, :, block(index, which, rows), :]

    back_side = pl.ds(pl.multiple_of(rep * (chans // 2), chans // 2), chans // 2)
    back_far = pl.ds(pl.multiple_of((1 - rep) * (chans // 2), chans // 2), chans // 2)

    def back_half(index, which, side):
        return back.at[side, block(index, which, back_cols)]

    def back_block(index, which):
        return back.at[:, block(index, which, back_cols)]

    step = half // STAGES
    up_rows = width // 2
    given = pl.ds(pl.multiple_of(rep * own_ff, own_ff), own_ff)
    taken = pl.ds(pl.multiple_of(2 * own_ff + rep * own_ff, own_ff), own_ff)
    turned = pl.ds(pl.multiple_of(3 * own_ff - rep * own_ff, own_ff), own_ff)

    def up_piece(part, units):
        return up.at[part * up_rows : (part + 1) * up_rows, units]

    def down_piece(part, units):
        return down.at[:, units, cuts[part] : cuts[part + 1]]

    cuts = [at * step for at in range(STAGES)] + [half - step // 2, half]
    stages = len(cuts) - 1
    early = 4
    flow = [("up", part, up_piece) for part in range(2)]
    flow += [("down", part, down_piece) for part in range(stages)]

    def cross_send(at, when=None):
        name, part, piece = flow[at]
        push((name, part, "z"), piece(part, given), {"fz": across}, piece(part, taken), when=when)

    def cross_turn(at, when):
        name, part, piece = flow[at]
        recv((name, part, "z"), piece(part, taken), when=when)
        push((name, part, "x"), piece(part, taken), to_rep, when=when)

    def cross_last(at):
        name, part, piece = flow[at]
        recv((name, part, "x"), piece(part, turned))

    def line_send(key, piece):
        push((key, 2), piece(0), {"fz": far}, when=middle)
        push((key, 3), piece(0), {"fz": far}, when=ends)
        push((key, 2), piece(0), {"fz": across}, when=middle)
        push((key, 1), piece(0), {"fz": near})

    def line_relay(key, piece):
        recv((key, 3), piece(3), when=middle)
        push((key, 3), piece(3), {"fz": near}, when=middle)

    def line_last(key, piece):
        recv((key, 3), piece(3), when=ends)

    local(0, [(hidden_hbm, stream.at[:, own_lanes])])
    push("hid", hidden_hbm, to_tp, stream.at[:, own_lanes])
    mine = block(0, fy, rows)
    local(
        1,
        [
            (hbm.at[:, side * cols : (side + 1) * cols], front.at[side, kind, mine, :])
            for side in range(2)
            for kind, hbm in enumerate((value_hbm, gate_hbm))
        ],
    )
    local(2, [(back_hbm, back_block(0, fy))])
    own_units = pl.ds(0, 2 * own_ff)
    local(3, [(up_hbm, up.at[:, own_units])])
    local(
        4,
        [
            (down_hbm.at[:, side * half : (side + 1) * half], down.at[side, own_units, :])
            for side in range(2)
        ],
    )

    local_wait(1, front_block(0, fy))
    line_send("zf", lambda index: front_half(index, fy, rep))
    push(("yf", 0, 0), front_half(0, fy, 0), to_fy)
    push(("yf", 0, 1), front_half(0, fy, 1), to_fy, when=middle)
    local_wait(2, back_block(0, fy))
    line_send("zb", lambda index: back_half(index, fy, back_side))

    halo[:, :HALO, :] = jnp.zeros((halo.shape[0], HALO, halo.shape[2]), f32)
    local_wait(0, stream.at[:, own_lanes])
    recv("hid", stream.at[:, pl.ds(pl.multiple_of((1 - tp) * half, half), half)])

    def norm_rows(at, carry):
        place = pl.ds(pl.multiple_of(at * 32, 32), 32)
        values = stream[place, :].astype(f32)
        scale = lax.rsqrt(jnp.sum(values * values, axis=-1, keepdims=True) / width + 1e-06)
        feat[0, place, :] = (values * scale * mix_gain[...]).astype(bf16)
        return carry

    lax.fori_loop(0, tokens // 32, norm_rows, 0)

    def front_on(index, when=None):
        push(("yf", index), front_half(index, fy, rep), to_fy, when=when)
        push(("xf", 0, index), front_half(index, fy, rep), to_rep, when=when)

    def front_turn(index):
        recv(("yf", index), front_half(index, 1 - fy, rep))
        push(("xf", 1, index), front_half(index, 1 - fy, rep), to_rep)

    def back_on(index):
        push(("yb", index), back_half(index, fy, back_side), to_fy)
        push(("xb", 0, index), back_half(index, fy, back_side), to_rep)

    def back_turn(index):
        recv(("yb", index), back_half(index, 1 - fy, back_side))
        push(("xb", 1, index), back_half(index, 1 - fy, back_side), to_rep)

    def front_cross():
        recv(("xf", 0, 1), front_half(1, fy, 1 - rep))
        push(("yf", "x"), front_half(1, fy, 1 - rep), to_fy)

    def back_cross():
        recv(("xb", 0, 1), back_half(1, fy, back_far))
        push(("yb", "x"), back_half(1, fy, back_far), to_fy)

    recv(("zf", 1), front_half(1, fy, rep))
    front_on(1)
    line_relay("zf", lambda index: front_half(index, fy, rep))
    front_on(3, middle)
    recv(("zf", 2), front_half(2, fy, rep))
    front_on(2)
    front_cross()
    local_wait(3, up.at[:, own_units])
    local_wait(4, down.at[:, own_units, :])
    line_last("zf", lambda index: front_half(index, fy, rep))
    front_on(3, ends)
    push(("yf", 0, 1), front_half(0, fy, 1), to_fy, when=ends)
    line_relay("zb", lambda index: back_half(index, fy, back_side))
    front_turn(2)
    front_turn(3)
    recv(("zb", 1), back_half(1, fy, back_side))
    back_on(1)
    recv(("zb", 2), back_half(2, fy, back_side))
    back_on(2)
    line_last("zb", lambda index: back_half(index, fy, back_side))
    back_on(3)
    pl.semaphore_signal(pair_sem, inc=1, device_id=to_tp, device_id_type=MESH)
    push(("yb", 0), back_block(0, fy), to_fy)
    pl.semaphore_wait(pair_sem, 1)
    for at in range(len(flow)):
        cross_send(at, None if at < early else middle)

    recv(("yf", 1), front_half(1, 1 - fy, rep))
    recv(("yf", 0, 0), front_half(0, 1 - fy, 0))
    recv(("yf", 0, 1), front_half(0, 1 - fy, 1))
    recv(("xf", 0, 2), front_half(2, fy, 1 - rep))
    recv(("xf", 1, 2), front_half(2, 1 - fy, 1 - rep))
    recv(("yf", "x"), front_half(1, 1 - fy, 1 - rep))
    recv(("xf", 0, 3), front_half(3, fy, 1 - rep))
    recv(("xf", 1, 3), front_half(3, 1 - fy, 1 - rep))

    sequences = tokens // LEN
    for side in range(2):
        value = jnp.dot(feat[0], front[side, 0], preferred_element_type=f32)
        gate = jnp.dot(feat[0], front[side, 1], preferred_element_type=f32)
        gated = value * jax.nn.sigmoid(gate)
        halo[:, HALO:, side * cols : (side + 1) * cols] = gated.reshape(sequences, LEN, cols)

    def filter_sequence(at, carry):
        place = pl.ds(pl.multiple_of(at * LEN, LEN), LEN)
        total = jnp.zeros((LEN, LANES), f32)
        squares = jnp.zeros((LEN, LANES), f32)
        for lane in range(chans // LANES):
            lanes = slice(lane * LANES, (lane + 1) * LANES)
            result = jnp.zeros((LEN, LANES), f32) + bias[:, lanes]
            for tap in range(KW):
                start = HALO - KW + 1 + tap
                result = result + taps[tap : tap + 1, lanes] * halo[at, start : start + LEN, lanes]
            filtered[place, lanes] = result
            total = total + result
            squares = squares + result * result
        stats[0, place, :] = total
        stats[1, place, :] = squares
        return carry

    middle_sequence = sequences - sequences // 2
    lax.fori_loop(0, middle_sequence, filter_sequence, 0)
    recv(("yb", 1), back_half(1, 1 - fy, back_side))
    back_cross()
    back_turn(2)
    lax.fori_loop(middle_sequence, sequences, filter_sequence, 0)
    back_turn(3)
    push("stats", stats, to_tp, stats_in)
    recv("stats", stats_in)

    def act_rows(at, carry):
        place = pl.ds(pl.multiple_of(at * 32, 32), 32)
        count = 2 * chans
        mean = jnp.sum(stats[0, place, :] + stats_in[0, place, :], axis=-1, keepdims=True) / count
        second_moment = (
            jnp.sum(stats[1, place, :] + stats_in[1, place, :], axis=-1, keepdims=True) / count
        )
        scale = lax.rsqrt(second_moment - mean * mean + 1e-05)
        centred = (filtered[place, :] - mean) * scale * chan_gain[...] + chan_bias[...]
        act[place, :] = (centred * jax.nn.sigmoid(centred)).astype(bf16)
        return carry

    lax.fori_loop(0, tokens // 32, act_rows, 0)

    recv(("yb", 0), back_block(0, 1 - fy))
    recv(("yb", "x"), back_half(1, 1 - fy, back_far))
    for index in range(2, LINE):
        recv(("xb", 0, index), back_half(index, fy, back_far))
        recv(("xb", 1, index), back_half(index, 1 - fy, back_far))

    def back_lanes(side, part):
        return pl.ds(pl.multiple_of(side * half + part * step, step), step)

    for part in range(STAGES):
        lanes = slice(part * step, (part + 1) * step)
        product = jnp.dot(act[...], back[:, back_lanes(1 - tp, part)], preferred_element_type=f32)
        mix_out[:, lanes] = product.astype(bf16)
    push("mix", mix_out, to_tp, mix_in)
    for part in range(STAGES):
        kept[part] = jnp.dot(act[...], back[:, back_lanes(tp, part)], preferred_element_type=f32)
    recv("mix", mix_in)

    def second_rows(at, carry):
        place = pl.ds(pl.multiple_of(at * 32, 32), 32)
        squares = jnp.zeros((32, LANES), f32)
        for part in range(STAGES):
            lanes = slice(part * step, (part + 1) * step)
            source = pl.ds(pl.multiple_of(tp * half + part * step, step), step)
            mixed = kept[part, place, :] + mix_in[place, lanes].astype(f32)
            value = (stream[place, source].astype(f32) + mixed).astype(bf16)
            second[place, lanes] = value
            value = value.astype(f32)
            value = value * value
            for lane in range(step // LANES):
                squares = squares + value[:, lane * LANES : (lane + 1) * LANES]
        square[place, :] = squares
        return carry

    lax.fori_loop(0, tokens // 32, second_rows, 0)
    push("square", square, to_tp, square_in)
    recv("square", square_in)

    def feed_rows(at, carry):
        place = pl.ds(pl.multiple_of(at * 32, 32), 32)
        mean = jnp.sum(square[place, :] + square_in[place, :], axis=-1, keepdims=True) / width
        scale = lax.rsqrt(mean + 1e-06)
        values = second[place, :].astype(f32) * scale * feed_gain[:, own_lanes]
        feat[0, place, own_lanes] = values.astype(bf16)
        return carry

    part_rows = tokens // 2

    def feat_part(index, part, lanes):
        return feat.at[index, part * part_rows : (part + 1) * part_rows, lanes]

    other_lanes = pl.ds(pl.multiple_of((1 - tp) * half, half), half)

    def share(index, part):
        push(("pair", index, part), feat_part(index, part, own_lanes), to_tp)

    def shared(index):
        for part in range(2):
            recv(("pair", index, part), feat_part(index, part, other_lanes))

    for part in range(2):
        lax.fori_loop(part * part_rows // 32, (part + 1) * part_rows // 32, feed_rows, 0)
        push(("line", part), feat_part(0, part, own_lanes), to_line, feat_part(1, part, own_lanes))
        push(("fy", part), feat_part(0, part, own_lanes), to_fy, feat_part(2, part, own_lanes))
        share(0, part)

    def up_slot(index, side):
        for part in range(2):
            lanes = slice((2 * side + part) * own_ff, (2 * side + part + 1) * own_ff)
            product = jnp.dot(feat[index], up[:, lanes], preferred_element_type=f32)
            hidden[index, :, lanes] = jnp.square(jnp.maximum(product, 0.0)).astype(bf16)

    for at in range(early - 1):
        cross_turn(at, ends)
    shared(0)
    up_slot(0, 0)
    cross_turn(0, middle)
    recv(("line", 0), feat_part(1, 0, own_lanes))
    push(("diag", 0), feat_part(1, 0, own_lanes), to_fy, feat_part(3, 0, own_lanes))
    share(1, 0)
    recv(("fy", 0), feat_part(2, 0, own_lanes))
    share(2, 0)
    cross_turn(1, middle)
    cross_turn(early - 1, ends)
    recv(("line", 1), feat_part(1, 1, own_lanes))
    share(1, 1)
    recv(("fy", 1), feat_part(2, 1, own_lanes))
    push(("diag", 1), feat_part(2, 1, own_lanes), to_line, feat_part(3, 1, own_lanes))
    for at in range(early, len(flow)):
        cross_send(at, ends)
    share(2, 1)
    shared(1)
    up_slot(1, 0)
    shared(2)
    up_slot(2, 0)
    cross_turn(2, middle)
    cross_last(0)
    cross_last(1)
    up_slot(0, 1)
    recv(("diag", 0), feat_part(3, 0, own_lanes))
    share(3, 0)
    up_slot(1, 1)
    cross_turn(3, middle)
    up_slot(2, 1)
    recv(("diag", 1), feat_part(3, 1, own_lanes))
    share(3, 1)
    shared(3)
    up_slot(3, 0)
    up_slot(3, 1)

    turn_rows = tokens * 3 // 10

    def home(stage, index):
        return index if index or stage % 2 == 0 else STAGES

    def span(stage):
        return slice(cuts[stage], cuts[stage + 1])

    def products(stage, index):
        lanes = span(stage)
        product = jnp.dot(hidden[index], down[1 - tp, :, lanes], preferred_element_type=f32)
        pair_out[index, :, lanes] = product.astype(bf16)
        push(
            ("sum", index, stage),
            pair_out.at[index, :, lanes],
            to_tp,
            pair_in.at[index, :, lanes],
        )
        product = jnp.dot(hidden[index], down[tp, :, lanes], preferred_element_type=f32)
        kept[home(stage, index), :, : cuts[stage + 1] - cuts[stage]] = product

    def paired(stage, index, first, last):
        lanes = span(stage)
        own = kept[home(stage, index), first:last, : cuts[stage + 1] - cuts[stage]]
        return own + pair_in[index, first:last, lanes].astype(f32)

    def finish(stage):
        lanes = span(stage)
        recv(("sum", 0, stage), pair_in.at[0, :, lanes])
        recv(("near", 0, stage), rep_in.at[:, lanes])
        recv(("near", 1, stage), fy_in.at[:, lanes])
        feed = paired(stage, 0, 0, tokens)
        feed = feed + rep_in[:, lanes].astype(f32) + fy_in[:, lanes].astype(f32)
        result[:, lanes] = (second[:, lanes].astype(f32) + feed).astype(bf16)
        local(5 + stage, [(result.at[:, lanes], out.at[:, lanes])])

    def send_far(stage):
        lanes = span(stage)
        recv(("sum", 3, stage), pair_in.at[3, :, lanes])
        plane_out[2, :, lanes] = paired(stage, 3, 0, tokens).astype(bf16)
        for part, (rows_of, device) in enumerate(
            ((slice(0, turn_rows), to_line), (slice(turn_rows, tokens), to_fy))
        ):
            push(
                ("far", part, stage),
                plane_out.at[2, rows_of, lanes],
                device,
                diag_in.at[rows_of, lanes],
            )

    def send_near(stage):
        lanes = span(stage)
        recv(("sum", 1, stage), pair_in.at[1, :, lanes])
        plane_out[0, :turn_rows, lanes] = paired(stage, 1, 0, turn_rows).astype(bf16)
        recv(("far", 1, stage), diag_in.at[turn_rows:, lanes])
        plane_out[0, turn_rows:, lanes] = (
            paired(stage, 1, turn_rows, tokens) + diag_in[turn_rows:, lanes].astype(f32)
        ).astype(bf16)
        push(("near", 0, stage), plane_out.at[0, :, lanes], to_line, rep_in.at[:, lanes])
        recv(("sum", 2, stage), pair_in.at[2, :, lanes])
        plane_out[1, turn_rows:, lanes] = paired(stage, 2, turn_rows, tokens).astype(bf16)
        recv(("far", 0, stage), diag_in.at[:turn_rows, lanes])
        plane_out[1, :turn_rows, lanes] = (
            paired(stage, 2, 0, turn_rows) + diag_in[:turn_rows, lanes].astype(f32)
        ).astype(bf16)
        push(("near", 1, stage), plane_out.at[1, :, lanes], to_fy, fy_in.at[:, lanes])

    cross_last(2)
    products(0, 3)
    products(0, 1)
    send_far(0)
    for stage in range(stages):
        last = stage + 1 == stages
        if not last:
            if stage == 0:
                cross_turn(early, None)
            cross_last(stage + 3)
            products(stage + 1, 3)
        products(stage, 2)
        products(stage, 0)
        if not last:
            send_far(stage + 1)
        send_near(stage)
        if early + stage + 1 < len(flow):
            cross_turn(early + stage + 1, None)
        if not last:
            products(stage + 1, 1)
        if stage:
            finish(stage - 1)
    finish(stages - 1)
    for stage in range(stages):
        lanes = span(stage)
        pltpu.make_async_copy(result.at[:, lanes], out.at[:, lanes], local_sem.at[5 + stage]).wait()

    for copy, when in sent:
        if when is None:
            copy().wait_send()
        else:
            pl.when(when)(lambda copy=copy: copy().wait_send())


def fused(*arrays):
    hidden_in, mix_gain, w_value, w_gate, taps, bias, gain, shift, w_back, feed_gain, w_up, w_down = arrays
    tokens, half = hidden_in.shape
    _, chans = w_value.shape
    width, ff = 2 * half, w_up.shape[1] // 2 * LINE
    bf16, f32 = jnp.bfloat16, jnp.float32
    vmem, hbm = pl.BlockSpec(memory_space=pltpu.VMEM), pl.BlockSpec(memory_space=pltpu.HBM)
    step = half // STAGES
    scratch = [
        ((tokens, width), bf16),
        ((4, tokens, width), bf16),
        ((2, 2, width, chans // 2), bf16),
        ((chans, width), bf16),
        ((tokens // LEN, HALO + LEN, chans), f32),
        ((tokens, chans), f32),
        ((tokens, chans), bf16),
        ((2, tokens, LANES), f32),
        ((2, tokens, LANES), f32),
        ((tokens, half), bf16),
        ((tokens, half), bf16),
        ((STAGES + 1, tokens, step), f32),
        ((tokens, half), bf16),
        ((tokens, LANES), f32),
        ((tokens, LANES), f32),
        ((width, ff), bf16),
        ((2, ff, half), bf16),
        ((4, tokens, ff), bf16),
        ((4, tokens, half), bf16),
        ((4, tokens, half), bf16),
        ((3, tokens, half), bf16),
        ((tokens, half), bf16),
        ((tokens, half), bf16),
        ((tokens, half), bf16),
    ]
    return pl.pallas_call(
        fused_kernel,
        out_shape=jax.ShapeDtypeStruct((tokens, half), bf16),
        in_specs=[hbm, vmem, hbm, hbm, vmem, vmem, vmem, vmem, hbm, vmem, hbm, hbm],
        out_specs=hbm,
        scratch_shapes=[pltpu.VMEM(shape, kind) for shape, kind in scratch]
        + [
            pltpu.SemaphoreType.DMA((6 + STAGES,)),
            pltpu.SemaphoreType.DMA((SENDS,)),
            pltpu.SemaphoreType.DMA((RECEIVES,)),
            pltpu.SemaphoreType.REGULAR,
        ],
        compiler_params=pltpu.CompilerParams(
            collective_id=0, has_side_effects=True, vmem_limit_bytes=67043328
        ),
    )(
        hidden_in,
        mix_gain[None],
        w_value,
        w_gate,
        taps,
        bias[None],
        gain[None],
        shift[None],
        w_back,
        feed_gain[None],
        w_up,
        w_down,
    )


def fits(mesh):
    return mesh.shape["rep"] == 2 and mesh.shape["fs"] == 2 * LINE and mesh.shape["tp"] == 2


def solution(mesh):
    n_rep, n_fs, n_tp = mesh.shape["rep"], mesh.shape["fs"], mesh.shape["tp"]
    split = Mesh(mesh.devices.reshape(n_rep, n_fs // 2, 2, n_tp), ("rep", "fz", "fy", "tp"))
    fs = ("fz", "fy")
    rows = P(("rep", "fz", "fy"), "tp")
    placed = (
        rows,
        P(),
        P(fs, "tp"),
        P(fs, "tp"),
        P(None, "tp"),
        P("tp"),
        P("tp"),
        P("tp"),
        P("tp", fs),
        P(),
        P(None, ("fz", "fy", "tp")),
        P(("fz", "fy", "tp"), None),
    )
    if fits(mesh):
        return jax.shard_map(fused, mesh=split, in_specs=placed, out_specs=rows, check_vma=False)
    return jax.shard_map(block, mesh=split, in_specs=placed, out_specs=rows, check_vma=False)
```

```python
import jax
import jax.numpy as jnp
from jax import lax
from jax.sharding import Mesh, PartitionSpec as P

from jax.experimental import pallas as pl
from jax.experimental.pallas import tpu as pltpu


KW = 31
LEN = 128


SWAP = [(0, 1), (1, 0)]


def swap(value, axis):
    return lax.ppermute(value, axis, SWAP)


def ordered(own, other, index, axis):
    first = jnp.where(index == 0, own, other)
    return jnp.concatenate([first, jnp.where(index == 0, other, own)], axis=axis)


def own_first(array, index, axis):
    half = array.shape[axis] // 2
    return jnp.concatenate(
        [
            lax.dynamic_slice_in_dim(array, index * half, half, axis),
            lax.dynamic_slice_in_dim(array, (1 - index) * half, half, axis),
        ],
        axis=axis,
    )


def rms_norm(stream, gain):
    values = stream.astype(jnp.float32)
    scaled = values * lax.rsqrt(jnp.mean(values * values, axis=-1, keepdims=True) + 1e-06)
    return (scaled * gain).astype(jnp.bfloat16)


def causal_filter(gated, conv_taps, conv_bias):
    channels = gated.shape[1]
    blocks = gated.reshape(gated.shape[0] // LEN, LEN, channels)
    padded = jnp.pad(blocks, ((0, 0), (KW - 1, 0), (0, 0)))
    result = jnp.zeros_like(blocks) + conv_bias
    for tap_index in range(KW):
        result = result + conv_taps[tap_index] * padded[:, tap_index : tap_index + LEN]
    return result.reshape(gated.shape)


def plane_slots(piece):
    half = piece.shape[0] // 2
    from_rep = swap(piece, "rep")
    from_fy = swap(piece, "fy")
    diag_low = swap(from_rep[:half], "fy")
    diag_high = swap(from_fy[half:], "rep")
    return [piece, from_rep, from_fy, jnp.concatenate([diag_low, diag_high], axis=0)]


def full_features(slot):
    return jnp.concatenate([slot, swap(slot, "tp")], axis=1)


def tp_reduced(left, right):
    width = right.shape[1] // 2
    sent = jnp.dot(left, right[:, width:], preferred_element_type=jnp.float32)
    kept = jnp.dot(left, right[:, :width], preferred_element_type=jnp.float32)
    return kept + swap(sent.astype(jnp.bfloat16), "tp").astype(jnp.float32)


def plane_reduced(compute):
    diag = compute(3)
    half = diag.shape[0] // 2
    via_rep = swap(diag[:half].astype(jnp.bfloat16), "rep").astype(jnp.float32)
    via_fy = swap(diag[half:].astype(jnp.bfloat16), "fy").astype(jnp.float32)
    for_rep = compute(1)
    for_rep = jnp.concatenate([for_rep[:half], for_rep[half:] + via_fy], axis=0)
    from_rep = swap(for_rep.astype(jnp.bfloat16), "rep")
    for_fy = compute(2)
    for_fy = jnp.concatenate([for_fy[:half] + via_rep, for_fy[half:]], axis=0)
    from_fy = swap(for_fy.astype(jnp.bfloat16), "fy")
    return compute(0) + from_rep.astype(jnp.float32) + from_fy.astype(jnp.float32)


def block(
    hidden_in,
    mix_gain,
    w_value,
    w_gate,
    conv_taps,
    conv_bias,
    chan_gain,
    chan_bias,
    w_back,
    feed_gain,
    w_up,
    w_down,
):
    rep, fy, tp = lax.axis_index("rep"), lax.axis_index("fy"), lax.axis_index("tp")
    n_fz = lax.axis_size("fz")
    n_rep, n_fy, n_tp = lax.axis_size("rep"), lax.axis_size("fy"), lax.axis_size("tp")
    parts = n_rep * n_fy
    mine, theirs = rep * n_fy + fy, rep * n_fy + 1 - fy
    rows, back_cols = w_value.shape[0], w_back.shape[1]
    own_ch = w_value.shape[1] // parts

    def columns(array, which):
        return lax.dynamic_slice_in_dim(array, which * own_ch, own_ch, array.ndim - 1)

    def front_pack(which):
        packed_out = lax.dynamic_slice_in_dim(w_back, which * own_ch, own_ch, 0)
        pieces = [packed_out]
        if back_cols > own_ch:
            pieces = [
                packed_out[:, at : at + own_ch] for at in range(0, back_cols, own_ch)
            ]
        elif back_cols < own_ch:
            pieces = [packed_out.reshape(-1, own_ch)]
        return jnp.concatenate([columns(w_value, which), columns(w_gate, which)] + pieces, axis=0)

    received = swap(front_pack(theirs), "fy")
    slots = plane_slots(hidden_in)
    pair = ordered(front_pack(mine)[None], received[None], fy, 0)
    front = lax.all_gather(pair, "fz", axis=0, tiled=True)
    blocks = n_fz * n_fy
    w_in = own_first(
        jnp.concatenate(
            [
                front[:, :rows].reshape(blocks * rows, own_ch),
                front[:, rows : 2 * rows].reshape(blocks * rows, own_ch),
            ],
            axis=1,
        ),
        tp,
        0,
    )
    if back_cols >= own_ch:
        whole_back = front[:, 2 * rows :].reshape(blocks * (back_cols // own_ch), own_ch, own_ch)
    else:
        whole_back = front[:, 2 * rows :].reshape(blocks, own_ch, back_cols)
    whole_back = own_first(
        whole_back.transpose(1, 0, 2).reshape(own_ch, blocks * back_cols), tp, 1
    )

    own_ff = w_up.shape[1] // n_rep
    up_part = own_first(lax.dynamic_slice_in_dim(w_up, rep * own_ff, own_ff, 1), tp, 0)
    down_part = own_first(lax.dynamic_slice_in_dim(w_down, rep * own_ff, own_ff, 0), tp, 1)
    up = lax.all_gather(up_part, "fz", axis=1, tiled=True)
    down = lax.all_gather(down_part, "fz", axis=0, tiled=True)

    taps, bias = columns(conv_taps, mine), columns(conv_bias, mine)
    gain, shift = columns(chan_gain, mine), columns(chan_bias, mine)

    tokens = hidden_in.shape[0]
    mix_rolled, feed_rolled = own_first(mix_gain, tp, 0), own_first(feed_gain, tp, 0)
    gated = []
    for slot in slots:
        normed = rms_norm(full_features(slot), mix_rolled)
        both = jnp.dot(normed, w_in, preferred_element_type=jnp.float32)
        gated.append(both[:, :own_ch] * jax.nn.sigmoid(both[:, own_ch:]))
    filtered = causal_filter(jnp.concatenate(gated, axis=0), taps, bias)
    stats = jnp.stack([jnp.sum(filtered, axis=1), jnp.sum(filtered * filtered, axis=1)])
    stats = stats.reshape(2, 4, tokens)
    stats = stats + swap(stats, "tp")
    other = swap(stats, "rep")
    stats = stats + jnp.stack([other[:, at] for at in (1, 0, 3, 2)], axis=1)
    other = swap(stats, "fy")
    stats = stats + jnp.stack([other[:, at] for at in (2, 3, 0, 1)], axis=1)
    stats = stats.reshape(2, 4 * tokens) / (own_ch * parts * n_tp)
    chan_mean = stats[0][:, None]
    chan_var = stats[1][:, None] - chan_mean * chan_mean
    centred = (filtered - chan_mean) * lax.rsqrt(chan_var + 1e-05) * gain + shift
    act = jax.nn.silu(centred).astype(jnp.bfloat16)

    def mixed_share(index):
        return tp_reduced(act[index * tokens : (index + 1) * tokens], whole_back)

    mixed = plane_reduced(mixed_share)
    second = (hidden_in.astype(jnp.float32) + mixed).astype(jnp.bfloat16)

    hidden = []
    for slot in plane_slots(second):
        normed = rms_norm(full_features(slot), feed_rolled)
        up_proj = jnp.dot(normed, up, preferred_element_type=jnp.float32)
        hidden.append(jnp.square(jax.nn.relu(up_proj)).astype(jnp.bfloat16))
    hidden = list(lax.optimization_barrier(tuple(hidden)))

    def feed_share(index):
        return tp_reduced(hidden[index], down)

    feed = plane_reduced(feed_share)
    return (second.astype(jnp.float32) + feed).astype(jnp.bfloat16)


MESH = pl.DeviceIdType.MESH
LINE = 4
STAGES = 4
SENDS = 200
RECEIVES = 140
LANES = 128
HALO = 32
SUBLANES = 8


def fused_kernel(
    hidden_hbm,
    mix_gain,
    value_hbm,
    gate_hbm,
    taps,
    bias,
    chan_gain,
    chan_bias,
    back_hbm,
    feed_gain,
    up_hbm,
    down_hbm,
    out,
    stream,
    feat,
    front,
    back,
    halo,
    filtered,
    act,
    stats,
    stats_in,
    mix_out,
    mix_in,
    kept,
    second,
    square,
    square_in,
    up,
    down,
    hidden,
    pair_out,
    pair_in,
    plane_out,
    diag_in,
    rep_in,
    fy_in,
    local_sem,
    send_sem,
    recv_sem,
    pair_sem,
):
    f32, bf16 = jnp.float32, jnp.bfloat16
    rep, z, fy, tp = (lax.axis_index(name) for name in ("rep", "fz", "fy", "tp"))
    low = z // (LINE // 2)
    near, far, across = z + 1 - 2 * lax.rem(z, 2), lax.rem(z + LINE // 2, LINE), LINE - 1 - z
    zs = (z, near, LINE // 2 - low, (LINE - 1) * (1 - low))
    middle = lax.rem(z, LINE - 1) != 0
    ends = lax.rem(z, LINE - 1) == 0
    to_rep, to_fy, to_tp = {"rep": 1 - rep}, {"fy": 1 - fy}, {"tp": 1 - tp}
    to_line = {"fz": near}
    tokens, half = second.shape
    rows, chans = value_hbm.shape
    cols = chans // 2
    back_cols = back_hbm.shape[1]
    own_ff = up_hbm.shape[1] // 2
    width = 2 * half
    sent, slots, result = [], {}, mix_in
    own_lanes = pl.ds(pl.multiple_of(tp * half, half), half)

    barrier = pltpu.get_barrier_semaphore()
    partners = [to_rep, to_fy, to_tp] + [{"fz": at} for at in (near, far, across)]
    for partner in partners:
        pl.semaphore_signal(barrier, inc=1, device_id=partner, device_id_type=MESH)
    pl.semaphore_wait(barrier, len(partners))

    def slot(key):
        if key not in slots:
            slots[key] = len(slots)
            assert len(slots) <= RECEIVES
        return recv_sem.at[slots[key]]

    def push(key, src, device, dst=None, when=None):
        place = send_sem.at[len(sent)]
        arrive = slot(key)

        def copy():
            return pltpu.make_async_remote_copy(
                src_ref=src,
                dst_ref=src if dst is None else dst,
                send_sem=place,
                recv_sem=arrive,
                device_id=device,
                device_id_type=MESH,
            )

        sent.append((copy, when))
        assert len(sent) <= SENDS
        if when is None:
            copy().start()
        else:
            pl.when(when)(lambda: copy().start())

    def recv(key, ref, when=None):
        arrive = slot(key)

        def wait():
            pltpu.make_async_remote_copy(
                src_ref=ref,
                dst_ref=ref,
                send_sem=send_sem.at[0],
                recv_sem=arrive,
                device_id=to_tp,
                device_id_type=MESH,
            ).wait_recv()

        if when is None:
            wait()
        else:
            pl.when(when)(wait)

    def local(index, pairs):
        for src, dst in pairs:
            pltpu.make_async_copy(src, dst, local_sem.at[index]).start()

    def local_wait(index, ref):
        pltpu.make_async_copy(ref, ref, local_sem.at[index]).wait()

    def block(index, which, size):
        return pl.ds(pl.multiple_of((zs[index] * 2 + which) * size, size), size)

    def front_half(index, which, side):
        return front.at[side, :, block(index, which, rows), :]

    def front_block(index, which):
        return front.at[:, :, block(index, which, rows), :]

    back_side = pl.ds(pl.multiple_of(rep * (chans // 2), chans // 2), chans // 2)
    back_far = pl.ds(pl.multiple_of((1 - rep) * (chans // 2), chans // 2), chans // 2)

    def back_half(index, which, side):
        return back.at[side, block(index, which, back_cols)]

    def back_block(index, which):
        return back.at[:, block(index, which, back_cols)]

    step = half // STAGES
    up_rows = width // 2
    given = pl.ds(pl.multiple_of(rep * own_ff, own_ff), own_ff)
    taken = pl.ds(pl.multiple_of(2 * own_ff + rep * own_ff, own_ff), own_ff)
    turned = pl.ds(pl.multiple_of(3 * own_ff - rep * own_ff, own_ff), own_ff)

    def up_piece(part, units):
        return up.at[part * up_rows : (part + 1) * up_rows, units]

    def down_piece(part, units):
        return down.at[:, units, cuts[part] : cuts[part + 1]]

    cuts = [at * step for at in range(STAGES)] + [half - step // 2, half]
    stages = len(cuts) - 1
    early = 4
    flow = [("up", part, up_piece) for part in range(2)]
    flow += [("down", part, down_piece) for part in range(stages)]

    def cross_send(at, when=None):
        name, part, piece = flow[at]
        push((name, part, "z"), piece(part, given), {"fz": across}, piece(part, taken), when=when)

    def cross_turn(at, when):
        name, part, piece = flow[at]
        recv((name, part, "z"), piece(part, taken), when=when)
        push((name, part, "x"), piece(part, taken), to_rep, when=when)

    def cross_last(at):
        name, part, piece = flow[at]
        recv((name, part, "x"), piece(part, turned))

    def line_send(key, piece):
        push((key, 2), piece(0), {"fz": far}, when=middle)
        push((key, 3), piece(0), {"fz": far}, when=ends)
        push((key, 2), piece(0), {"fz": across}, when=middle)
        push((key, 1), piece(0), {"fz": near})

    def line_relay(key, piece):
        recv((key, 3), piece(3), when=middle)
        push((key, 3), piece(3), {"fz": near}, when=middle)

    def line_last(key, piece):
        recv((key, 3), piece(3), when=ends)

    local(0, [(hidden_hbm, stream.at[:, own_lanes])])
    push("hid", hidden_hbm, to_tp, stream.at[:, own_lanes])
    mine = block(0, fy, rows)
    local(
        1,
        [
            (hbm.at[:, side * cols : (side + 1) * cols], front.at[side, kind, mine, :])
            for side in range(2)
            for kind, hbm in enumerate((value_hbm, gate_hbm))
        ],
    )
    local(2, [(back_hbm, back_block(0, fy))])
    own_units = pl.ds(0, 2 * own_ff)
    local(3, [(up_hbm, up.at[:, own_units])])
    local(
        4,
        [
            (down_hbm.at[:, side * half : (side + 1) * half], down.at[side, own_units, :])
            for side in range(2)
        ],
    )

    local_wait(1, front_block(0, fy))
    line_send("zf", lambda index: front_half(index, fy, rep))
    push(("yf", 0, 0), front_half(0, fy, 0), to_fy)
    push(("yf", 0, 1), front_half(0, fy, 1), to_fy, when=middle)
    local_wait(2, back_block(0, fy))
    line_send("zb", lambda index: back_half(index, fy, back_side))

    halo[:, :HALO, :] = jnp.zeros((halo.shape[0], HALO, halo.shape[2]), f32)
    local_wait(0, stream.at[:, own_lanes])
    recv("hid", stream.at[:, pl.ds(pl.multiple_of((1 - tp) * half, half), half)])

    def norm_rows(at, carry):
        place = pl.ds(pl.multiple_of(at * 32, 32), 32)
        values = stream[place, :].astype(f32)
        scale = lax.rsqrt(jnp.sum(values * values, axis=-1, keepdims=True) / width + 1e-06)
        feat[0, place, :] = (values * scale * mix_gain[...]).astype(bf16)
        return carry

    lax.fori_loop(0, tokens // 32, norm_rows, 0)

    def front_on(index, when=None):
        push(("yf", index), front_half(index, fy, rep), to_fy, when=when)
        push(("xf", 0, index), front_half(index, fy, rep), to_rep, when=when)

    def front_turn(index):
        recv(("yf", index), front_half(index, 1 - fy, rep))
        push(("xf", 1, index), front_half(index, 1 - fy, rep), to_rep)

    def back_on(index):
        push(("yb", index), back_half(index, fy, back_side), to_fy)
        push(("xb", 0, index), back_half(index, fy, back_side), to_rep)

    def back_turn(index):
        recv(("yb", index), back_half(index, 1 - fy, back_side))
        push(("xb", 1, index), back_half(index, 1 - fy, back_side), to_rep)

    def front_cross():
        recv(("xf", 0, 1), front_half(1, fy, 1 - rep))
        push(("yf", "x"), front.at[1 - rep, 0, block(1, fy, rows), :], to_fy)

    def back_cross():
        recv(("xb", 0, 1), back_half(1, fy, back_far))
        push(("yb", "x"), back_half(1, fy, back_far), to_fy)

    recv(("zf", 1), front_half(1, fy, rep))
    front_on(1)
    line_relay("zf", lambda index: front_half(index, fy, rep))
    front_on(3, middle)
    recv(("zf", 2), front_half(2, fy, rep))
    front_on(2)
    recv(("yf", 1), front_half(1, 1 - fy, rep))
    push(("xf", "y"), front.at[rep, 1, block(1, 1 - fy, rows), :], to_rep)
    local_wait(3, up.at[:, own_units])
    local_wait(4, down.at[:, own_units, :])
    line_last("zf", lambda index: front_half(index, fy, rep))
    front_on(3, ends)
    front_cross()
    push(("yf", 0, 1), front_half(0, fy, 1), to_fy, when=ends)
    line_relay("zb", lambda index: back_half(index, fy, back_side))
    front_turn(2)
    front_turn(3)
    recv(("zb", 1), back_half(1, fy, back_side))
    back_on(1)
    recv(("zb", 2), back_half(2, fy, back_side))
    back_on(2)
    line_last("zb", lambda index: back_half(index, fy, back_side))
    back_on(3)
    pl.semaphore_signal(pair_sem, inc=1, device_id=to_tp, device_id_type=MESH)
    push(("yb", 0), back_block(0, fy), to_fy)
    pl.semaphore_wait(pair_sem, 1)
    for at in range(len(flow)):
        cross_send(at, None if at < early else middle)

    recv(("yf", 0, 0), front_half(0, 1 - fy, 0))
    recv(("yf", 0, 1), front_half(0, 1 - fy, 1))
    recv(("xf", 0, 2), front_half(2, fy, 1 - rep))
    recv(("xf", 1, 2), front_half(2, 1 - fy, 1 - rep))
    recv(("yf", "x"), front.at[1 - rep, 0, block(1, 1 - fy, rows), :])
    recv(("xf", "y"), front.at[1 - rep, 1, block(1, 1 - fy, rows), :])
    recv(("xf", 0, 3), front_half(3, fy, 1 - rep))
    recv(("xf", 1, 3), front_half(3, 1 - fy, 1 - rep))

    sequences = tokens // LEN
    for side in range(2):
        value = jnp.dot(feat[0], front[side, 0], preferred_element_type=f32)
        gate = jnp.dot(feat[0], front[side, 1], preferred_element_type=f32)
        gated = value * jax.nn.sigmoid(gate)
        halo[:, HALO:, side * cols : (side + 1) * cols] = gated.reshape(sequences, LEN, cols)

    def filter_sequence(at, carry):
        place = pl.ds(pl.multiple_of(at * LEN, LEN), LEN)
        total = jnp.zeros((LEN, LANES), f32)
        squares = jnp.zeros((LEN, LANES), f32)
        for lane in range(chans // LANES):
            lanes = slice(lane * LANES, (lane + 1) * LANES)
            result = jnp.zeros((LEN, LANES), f32) + bias[:, lanes]
            for shift in range(SUBLANES):
                size = LEN + SUBLANES if shift else LEN
                part = None
                for start in range(0, HALO + 1, SUBLANES):
                    tap = start + shift - (HALO - KW + 1)
                    if 0 <= tap < KW:
                        term = taps[tap : tap + 1, lanes] * halo[at, start : start + size, lanes]
                        part = term if part is None else part + term
                if shift:
                    part = pltpu.roll(part, size - shift, 0)[:LEN]
                result = result + part
            filtered[place, lanes] = result
            total = total + result
            squares = squares + result * result
        stats[0, place, :] = total
        stats[1, place, :] = squares
        return carry

    middle_sequence = sequences - sequences // 2
    lax.fori_loop(0, middle_sequence, filter_sequence, 0)
    recv(("yb", 1), back_half(1, 1 - fy, back_side))
    back_cross()
    back_turn(2)
    lax.fori_loop(middle_sequence, sequences, filter_sequence, 0)
    back_turn(3)
    push("stats", stats, to_tp, stats_in)
    recv("stats", stats_in)

    def act_rows(at, carry):
        place = pl.ds(pl.multiple_of(at * 32, 32), 32)
        count = 2 * chans
        mean = jnp.sum(stats[0, place, :] + stats_in[0, place, :], axis=-1, keepdims=True) / count
        second_moment = (
            jnp.sum(stats[1, place, :] + stats_in[1, place, :], axis=-1, keepdims=True) / count
        )
        scale = lax.rsqrt(second_moment - mean * mean + 1e-05)
        centred = (filtered[place, :] - mean) * scale * chan_gain[...] + chan_bias[...]
        act[place, :] = (centred * jax.nn.sigmoid(centred)).astype(bf16)
        return carry

    lax.fori_loop(0, tokens // 32, act_rows, 0)

    recv(("yb", 0), back_block(0, 1 - fy))
    recv(("yb", "x"), back_half(1, 1 - fy, back_far))
    for index in range(2, LINE):
        recv(("xb", 0, index), back_half(index, fy, back_far))
        recv(("xb", 1, index), back_half(index, 1 - fy, back_far))

    def back_lanes(side, part):
        return pl.ds(pl.multiple_of(side * half + part * step, step), step)

    for part in range(STAGES):
        lanes = slice(part * step, (part + 1) * step)
        product = jnp.dot(act[...], back[:, back_lanes(1 - tp, part)], preferred_element_type=f32)
        mix_out[:, lanes] = product.astype(bf16)
    push("mix", mix_out, to_tp, mix_in)
    for part in range(STAGES):
        kept[part] = jnp.dot(act[...], back[:, back_lanes(tp, part)], preferred_element_type=f32)
    recv("mix", mix_in)

    def second_rows(at, carry):
        place = pl.ds(pl.multiple_of(at * 32, 32), 32)
        squares = jnp.zeros((32, LANES), f32)
        for part in range(STAGES):
            lanes = slice(part * step, (part + 1) * step)
            source = pl.ds(pl.multiple_of(tp * half + part * step, step), step)
            mixed = kept[part, place, :] + mix_in[place, lanes].astype(f32)
            value = (stream[place, source].astype(f32) + mixed).astype(bf16)
            second[place, lanes] = value
            value = value.astype(f32)
            value = value * value
            for lane in range(step // LANES):
                squares = squares + value[:, lane * LANES : (lane + 1) * LANES]
        square[place, :] = squares
        return carry

    lax.fori_loop(0, tokens // 32, second_rows, 0)
    push("square", square, to_tp, square_in)
    recv("square", square_in)

    def feed_rows(at, carry):
        place = pl.ds(pl.multiple_of(at * 32, 32), 32)
        mean = jnp.sum(square[place, :] + square_in[place, :], axis=-1, keepdims=True) / width
        scale = lax.rsqrt(mean + 1e-06)
        values = second[place, :].astype(f32) * scale * feed_gain[:, own_lanes]
        feat[0, place, own_lanes] = values.astype(bf16)
        return carry

    part_rows = tokens // 2

    bounds = {index: (0, part_rows, tokens) for index in range(3)}
    bounds[3] = (0, part_rows, part_rows + part_rows // 2, tokens)

    def feat_part(index, part, lanes, like=None):
        edges = bounds[index if like is None else like]
        return feat.at[index, edges[part] : edges[part + 1], lanes]

    other_lanes = pl.ds(pl.multiple_of((1 - tp) * half, half), half)

    def share(index, part):
        push(("pair", index, part), feat_part(index, part, own_lanes), to_tp)

    def shared(index, part):
        recv(("pair", index, part), feat_part(index, part, other_lanes))

    for part in range(2):
        lax.fori_loop(part * part_rows // 32, (part + 1) * part_rows // 32, feed_rows, 0)
        push(("line", part), feat_part(0, part, own_lanes), to_line, feat_part(1, part, own_lanes))
        push(("fy", part), feat_part(0, part, own_lanes), to_fy, feat_part(2, part, own_lanes))
        share(0, part)

    def up_slot(index, side, part=None):
        first, last = (0, tokens) if part is None else bounds[index][part : part + 2]
        for piece in range(2):
            lanes = slice((2 * side + piece) * own_ff, (2 * side + piece + 1) * own_ff)
            product = jnp.dot(
                feat[index, first:last, :], up[:, lanes], preferred_element_type=f32
            )
            product = jnp.square(jnp.maximum(product, 0.0))
            hidden[index, first:last, lanes] = product.astype(bf16)

    for at in range(early - 1):
        cross_turn(at, ends)
    shared(0, 0)
    shared(0, 1)
    up_slot(0, 0)
    cross_turn(0, middle)
    recv(("line", 0), feat_part(1, 0, own_lanes))
    push(("diag", 0), feat_part(1, 0, own_lanes), to_fy, feat_part(3, 0, own_lanes))
    share(1, 0)
    recv(("fy", 0), feat_part(2, 0, own_lanes))
    share(2, 0)
    cross_turn(1, middle)
    cross_turn(early - 1, ends)
    recv(("line", 1), feat_part(1, 1, own_lanes))
    share(1, 1)
    recv(("fy", 1), feat_part(2, 1, own_lanes))
    for part in (1, 2):
        push(
            ("diag", part),
            feat_part(2, part, own_lanes, 3),
            to_line,
            feat_part(3, part, own_lanes),
        )
    for at in range(early, len(flow)):
        cross_send(at, ends)
    share(2, 1)
    shared(1, 0)
    shared(1, 1)
    up_slot(1, 0)
    shared(2, 0)
    shared(2, 1)
    up_slot(2, 0)
    cross_turn(2, middle)
    cross_last(0)
    cross_last(1)
    up_slot(0, 1)
    recv(("diag", 0), feat_part(3, 0, own_lanes))
    share(3, 0)
    up_slot(1, 1)
    cross_turn(3, middle)
    up_slot(2, 1)
    shared(3, 0)
    for side in range(2):
        up_slot(3, side, 0)
    for part in (1, 2):
        recv(("diag", part), feat_part(3, part, own_lanes))
        share(3, part)
    for part in (1, 2):
        shared(3, part)
        for side in range(2):
            up_slot(3, side, part)

    turn_rows = tokens * 3 // 10

    def home(stage, index):
        return index if index or stage % 2 == 0 else STAGES

    def span(stage):
        return slice(cuts[stage], cuts[stage + 1])

    def products(stage, index):
        lanes = span(stage)
        product = jnp.dot(hidden[index], down[1 - tp, :, lanes], preferred_element_type=f32)
        pair_out[index, :, lanes] = product.astype(bf16)
        push(
            ("sum", index, stage),
            pair_out.at[index, :, lanes],
            to_tp,
            pair_in.at[index, :, lanes],
        )
        product = jnp.dot(hidden[index], down[tp, :, lanes], preferred_element_type=f32)
        kept[home(stage, index), :, : cuts[stage + 1] - cuts[stage]] = product

    def paired(stage, index, first, last):
        lanes = span(stage)
        own = kept[home(stage, index), first:last, : cuts[stage + 1] - cuts[stage]]
        return own + pair_in[index, first:last, lanes].astype(f32)

    def finish(stage):
        lanes = span(stage)
        recv(("sum", 0, stage), pair_in.at[0, :, lanes])
        recv(("near", 0, stage), rep_in.at[:, lanes])
        recv(("near", 1, stage), fy_in.at[:, lanes])
        feed = paired(stage, 0, 0, tokens)
        feed = feed + rep_in[:, lanes].astype(f32) + fy_in[:, lanes].astype(f32)
        result[:, lanes] = (second[:, lanes].astype(f32) + feed).astype(bf16)
        local(5 + stage, [(result.at[:, lanes], out.at[:, lanes])])

    def send_far(stage):
        lanes = span(stage)
        recv(("sum", 3, stage), pair_in.at[3, :, lanes])
        plane_out[2, :, lanes] = paired(stage, 3, 0, tokens).astype(bf16)
        for part, (rows_of, device) in enumerate(
            ((slice(0, turn_rows), to_line), (slice(turn_rows, tokens), to_fy))
        ):
            push(
                ("far", part, stage),
                plane_out.at[2, rows_of, lanes],
                device,
                diag_in.at[rows_of, lanes],
            )

    def send_near(stage):
        lanes = span(stage)
        recv(("sum", 1, stage), pair_in.at[1, :, lanes])
        plane_out[0, :turn_rows, lanes] = paired(stage, 1, 0, turn_rows).astype(bf16)
        recv(("far", 1, stage), diag_in.at[turn_rows:, lanes])
        plane_out[0, turn_rows:, lanes] = (
            paired(stage, 1, turn_rows, tokens) + diag_in[turn_rows:, lanes].astype(f32)
        ).astype(bf16)
        push(("near", 0, stage), plane_out.at[0, :, lanes], to_line, rep_in.at[:, lanes])
        recv(("sum", 2, stage), pair_in.at[2, :, lanes])
        plane_out[1, turn_rows:, lanes] = paired(stage, 2, turn_rows, tokens).astype(bf16)
        recv(("far", 0, stage), diag_in.at[:turn_rows, lanes])
        plane_out[1, :turn_rows, lanes] = (
            paired(stage, 2, 0, turn_rows) + diag_in[:turn_rows, lanes].astype(f32)
        ).astype(bf16)
        push(("near", 1, stage), plane_out.at[1, :, lanes], to_fy, fy_in.at[:, lanes])

    cross_last(2)
    products(0, 3)
    products(0, 1)
    send_far(0)
    for stage in range(stages):
        last = stage + 1 == stages
        if not last:
            if stage == 0:
                cross_turn(early, None)
            cross_last(stage + 3)
            products(stage + 1, 3)
        products(stage, 2)
        products(stage, 0)
        if not last:
            send_far(stage + 1)
        send_near(stage)
        if early + stage + 1 < len(flow):
            cross_turn(early + stage + 1, None)
        if not last:
            products(stage + 1, 1)
        if stage:
            finish(stage - 1)
    finish(stages - 1)
    for stage in range(stages):
        lanes = span(stage)
        pltpu.make_async_copy(result.at[:, lanes], out.at[:, lanes], local_sem.at[5 + stage]).wait()

    for copy, when in sent:
        if when is None:
            copy().wait_send()
        else:
            pl.when(when)(lambda copy=copy: copy().wait_send())


def fused(*arrays):
    hidden_in, mix_gain, w_value, w_gate, taps, bias, gain, shift, w_back, feed_gain, w_up, w_down = arrays
    tokens, half = hidden_in.shape
    _, chans = w_value.shape
    width, ff = 2 * half, w_up.shape[1] // 2 * LINE
    bf16, f32 = jnp.bfloat16, jnp.float32
    vmem, hbm = pl.BlockSpec(memory_space=pltpu.VMEM), pl.BlockSpec(memory_space=pltpu.HBM)
    step = half // STAGES
    scratch = [
        ((tokens, width), bf16),
        ((4, tokens, width), bf16),
        ((2, 2, width, chans // 2), bf16),
        ((chans, width), bf16),
        ((tokens // LEN, HALO + LEN, chans), f32),
        ((tokens, chans), f32),
        ((tokens, chans), bf16),
        ((2, tokens, LANES), f32),
        ((2, tokens, LANES), f32),
        ((tokens, half), bf16),
        ((tokens, half), bf16),
        ((STAGES + 1, tokens, step), f32),
        ((tokens, half), bf16),
        ((tokens, LANES), f32),
        ((tokens, LANES), f32),
        ((width, ff), bf16),
        ((2, ff, half), bf16),
        ((4, tokens, ff), bf16),
        ((4, tokens, half), bf16),
        ((4, tokens, half), bf16),
        ((3, tokens, half), bf16),
        ((tokens, half), bf16),
        ((tokens, half), bf16),
        ((tokens, half), bf16),
    ]
    return pl.pallas_call(
        fused_kernel,
        out_shape=jax.ShapeDtypeStruct((tokens, half), bf16),
        in_specs=[hbm, vmem, hbm, hbm, vmem, vmem, vmem, vmem, hbm, vmem, hbm, hbm],
        out_specs=hbm,
        scratch_shapes=[pltpu.VMEM(shape, kind) for shape, kind in scratch]
        + [
            pltpu.SemaphoreType.DMA((6 + STAGES,)),
            pltpu.SemaphoreType.DMA((SENDS,)),
            pltpu.SemaphoreType.DMA((RECEIVES,)),
            pltpu.SemaphoreType.REGULAR,
        ],
        compiler_params=pltpu.CompilerParams(
            collective_id=0, has_side_effects=True, vmem_limit_bytes=67043328
        ),
    )(
        hidden_in,
        mix_gain[None],
        w_value,
        w_gate,
        taps,
        bias[None],
        gain[None],
        shift[None],
        w_back,
        feed_gain[None],
        w_up,
        w_down,
    )


def fits(mesh):
    return mesh.shape["rep"] == 2 and mesh.shape["fs"] == 2 * LINE and mesh.shape["tp"] == 2


def solution(mesh):
    n_rep, n_fs, n_tp = mesh.shape["rep"], mesh.shape["fs"], mesh.shape["tp"]
    split = Mesh(mesh.devices.reshape(n_rep, n_fs // 2, 2, n_tp), ("rep", "fz", "fy", "tp"))
    fs = ("fz", "fy")
    rows = P(("rep", "fz", "fy"), "tp")
    placed = (
        rows,
        P(),
        P(fs, "tp"),
        P(fs, "tp"),
        P(None, "tp"),
        P("tp"),
        P("tp"),
        P("tp"),
        P("tp", fs),
        P(),
        P(None, ("fz", "fy", "tp")),
        P(("fz", "fy", "tp"), None),
    )
    if fits(mesh):
        return jax.shard_map(fused, mesh=split, in_specs=placed, out_specs=rows, check_vma=False)
    return jax.shard_map(block, mesh=split, in_specs=placed, out_specs=rows, check_vma=False)
```

```python
import jax
import jax.numpy as jnp
from jax import lax
from jax.sharding import Mesh, PartitionSpec as P

from jax.experimental import pallas as pl
from jax.experimental.pallas import tpu as pltpu


KW = 31
LEN = 128


SWAP = [(0, 1), (1, 0)]


def swap(value, axis):
    return lax.ppermute(value, axis, SWAP)


def ordered(own, other, index, axis):
    first = jnp.where(index == 0, own, other)
    return jnp.concatenate([first, jnp.where(index == 0, other, own)], axis=axis)


def own_first(array, index, axis):
    half = array.shape[axis] // 2
    return jnp.concatenate(
        [
            lax.dynamic_slice_in_dim(array, index * half, half, axis),
            lax.dynamic_slice_in_dim(array, (1 - index) * half, half, axis),
        ],
        axis=axis,
    )


def rms_norm(stream, gain):
    values = stream.astype(jnp.float32)
    scaled = values * lax.rsqrt(jnp.mean(values * values, axis=-1, keepdims=True) + 1e-06)
    return (scaled * gain).astype(jnp.bfloat16)


def causal_filter(gated, conv_taps, conv_bias):
    channels = gated.shape[1]
    blocks = gated.reshape(gated.shape[0] // LEN, LEN, channels)
    padded = jnp.pad(blocks, ((0, 0), (KW - 1, 0), (0, 0)))
    result = jnp.zeros_like(blocks) + conv_bias
    for tap_index in range(KW):
        result = result + conv_taps[tap_index] * padded[:, tap_index : tap_index + LEN]
    return result.reshape(gated.shape)


def plane_slots(piece):
    half = piece.shape[0] // 2
    from_rep = swap(piece, "rep")
    from_fy = swap(piece, "fy")
    diag_low = swap(from_rep[:half], "fy")
    diag_high = swap(from_fy[half:], "rep")
    return [piece, from_rep, from_fy, jnp.concatenate([diag_low, diag_high], axis=0)]


def full_features(slot):
    return jnp.concatenate([slot, swap(slot, "tp")], axis=1)


def tp_reduced(left, right):
    width = right.shape[1] // 2
    sent = jnp.dot(left, right[:, width:], preferred_element_type=jnp.float32)
    kept = jnp.dot(left, right[:, :width], preferred_element_type=jnp.float32)
    return kept + swap(sent.astype(jnp.bfloat16), "tp").astype(jnp.float32)


def plane_reduced(compute):
    diag = compute(3)
    half = diag.shape[0] // 2
    via_rep = swap(diag[:half].astype(jnp.bfloat16), "rep").astype(jnp.float32)
    via_fy = swap(diag[half:].astype(jnp.bfloat16), "fy").astype(jnp.float32)
    for_rep = compute(1)
    for_rep = jnp.concatenate([for_rep[:half], for_rep[half:] + via_fy], axis=0)
    from_rep = swap(for_rep.astype(jnp.bfloat16), "rep")
    for_fy = compute(2)
    for_fy = jnp.concatenate([for_fy[:half] + via_rep, for_fy[half:]], axis=0)
    from_fy = swap(for_fy.astype(jnp.bfloat16), "fy")
    return compute(0) + from_rep.astype(jnp.float32) + from_fy.astype(jnp.float32)


def block(
    hidden_in,
    mix_gain,
    w_value,
    w_gate,
    conv_taps,
    conv_bias,
    chan_gain,
    chan_bias,
    w_back,
    feed_gain,
    w_up,
    w_down,
):
    rep, fy, tp = lax.axis_index("rep"), lax.axis_index("fy"), lax.axis_index("tp")
    n_fz = lax.axis_size("fz")
    n_rep, n_fy, n_tp = lax.axis_size("rep"), lax.axis_size("fy"), lax.axis_size("tp")
    parts = n_rep * n_fy
    mine, theirs = rep * n_fy + fy, rep * n_fy + 1 - fy
    rows, back_cols = w_value.shape[0], w_back.shape[1]
    own_ch = w_value.shape[1] // parts

    def columns(array, which):
        return lax.dynamic_slice_in_dim(array, which * own_ch, own_ch, array.ndim - 1)

    def front_pack(which):
        packed_out = lax.dynamic_slice_in_dim(w_back, which * own_ch, own_ch, 0)
        pieces = [packed_out]
        if back_cols > own_ch:
            pieces = [
                packed_out[:, at : at + own_ch] for at in range(0, back_cols, own_ch)
            ]
        elif back_cols < own_ch:
            pieces = [packed_out.reshape(-1, own_ch)]
        return jnp.concatenate([columns(w_value, which), columns(w_gate, which)] + pieces, axis=0)

    received = swap(front_pack(theirs), "fy")
    slots = plane_slots(hidden_in)
    pair = ordered(front_pack(mine)[None], received[None], fy, 0)
    front = lax.all_gather(pair, "fz", axis=0, tiled=True)
    blocks = n_fz * n_fy
    w_in = own_first(
        jnp.concatenate(
            [
                front[:, :rows].reshape(blocks * rows, own_ch),
                front[:, rows : 2 * rows].reshape(blocks * rows, own_ch),
            ],
            axis=1,
        ),
        tp,
        0,
    )
    if back_cols >= own_ch:
        whole_back = front[:, 2 * rows :].reshape(blocks * (back_cols // own_ch), own_ch, own_ch)
    else:
        whole_back = front[:, 2 * rows :].reshape(blocks, own_ch, back_cols)
    whole_back = own_first(
        whole_back.transpose(1, 0, 2).reshape(own_ch, blocks * back_cols), tp, 1
    )

    own_ff = w_up.shape[1] // n_rep
    up_part = own_first(lax.dynamic_slice_in_dim(w_up, rep * own_ff, own_ff, 1), tp, 0)
    down_part = own_first(lax.dynamic_slice_in_dim(w_down, rep * own_ff, own_ff, 0), tp, 1)
    up = lax.all_gather(up_part, "fz", axis=1, tiled=True)
    down = lax.all_gather(down_part, "fz", axis=0, tiled=True)

    taps, bias = columns(conv_taps, mine), columns(conv_bias, mine)
    gain, shift = columns(chan_gain, mine), columns(chan_bias, mine)

    tokens = hidden_in.shape[0]
    mix_rolled, feed_rolled = own_first(mix_gain, tp, 0), own_first(feed_gain, tp, 0)
    gated = []
    for slot in slots:
        normed = rms_norm(full_features(slot), mix_rolled)
        both = jnp.dot(normed, w_in, preferred_element_type=jnp.float32)
        gated.append(both[:, :own_ch] * jax.nn.sigmoid(both[:, own_ch:]))
    filtered = causal_filter(jnp.concatenate(gated, axis=0), taps, bias)
    stats = jnp.stack([jnp.sum(filtered, axis=1), jnp.sum(filtered * filtered, axis=1)])
    stats = stats.reshape(2, 4, tokens)
    stats = stats + swap(stats, "tp")
    other = swap(stats, "rep")
    stats = stats + jnp.stack([other[:, at] for at in (1, 0, 3, 2)], axis=1)
    other = swap(stats, "fy")
    stats = stats + jnp.stack([other[:, at] for at in (2, 3, 0, 1)], axis=1)
    stats = stats.reshape(2, 4 * tokens) / (own_ch * parts * n_tp)
    chan_mean = stats[0][:, None]
    chan_var = stats[1][:, None] - chan_mean * chan_mean
    centred = (filtered - chan_mean) * lax.rsqrt(chan_var + 1e-05) * gain + shift
    act = jax.nn.silu(centred).astype(jnp.bfloat16)

    def mixed_share(index):
        return tp_reduced(act[index * tokens : (index + 1) * tokens], whole_back)

    mixed = plane_reduced(mixed_share)
    second = (hidden_in.astype(jnp.float32) + mixed).astype(jnp.bfloat16)

    hidden = []
    for slot in plane_slots(second):
        normed = rms_norm(full_features(slot), feed_rolled)
        up_proj = jnp.dot(normed, up, preferred_element_type=jnp.float32)
        hidden.append(jnp.square(jax.nn.relu(up_proj)).astype(jnp.bfloat16))
    hidden = list(lax.optimization_barrier(tuple(hidden)))

    def feed_share(index):
        return tp_reduced(hidden[index], down)

    feed = plane_reduced(feed_share)
    return (second.astype(jnp.float32) + feed).astype(jnp.bfloat16)


MESH = pl.DeviceIdType.MESH
LINE = 4
STAGES = 4
SENDS = 200
RECEIVES = 140
LANES = 128
HALO = 32
SUBLANES = 8


def fused_kernel(
    hidden_hbm,
    mix_gain,
    value_hbm,
    gate_hbm,
    taps,
    bias,
    chan_gain,
    chan_bias,
    back_hbm,
    feed_gain,
    up_hbm,
    down_hbm,
    out,
    stream,
    feat,
    front,
    back,
    halo,
    filtered,
    act,
    stats,
    stats_in,
    mix_out,
    mix_in,
    kept,
    second,
    square,
    square_in,
    up,
    down,
    hidden,
    pair_out,
    pair_in,
    plane_out,
    diag_in,
    rep_in,
    fy_in,
    local_sem,
    send_sem,
    recv_sem,
    pair_sem,
):
    f32, bf16 = jnp.float32, jnp.bfloat16
    rep, z, fy, tp = (lax.axis_index(name) for name in ("rep", "fz", "fy", "tp"))
    low = z // (LINE // 2)
    near, far, across = z + 1 - 2 * lax.rem(z, 2), lax.rem(z + LINE // 2, LINE), LINE - 1 - z
    zs = (z, near, LINE // 2 - low, (LINE - 1) * (1 - low))
    middle = lax.rem(z, LINE - 1) != 0
    ends = lax.rem(z, LINE - 1) == 0
    to_rep, to_fy, to_tp = {"rep": 1 - rep}, {"fy": 1 - fy}, {"tp": 1 - tp}
    to_line = {"fz": near}
    tokens, half = second.shape
    rows, chans = value_hbm.shape
    cols = chans // 2
    back_cols = back_hbm.shape[1]
    own_ff = up_hbm.shape[1] // 2
    width = 2 * half
    sent, slots, result = [], {}, mix_in
    own_lanes = pl.ds(pl.multiple_of(tp * half, half), half)

    barrier = pltpu.get_barrier_semaphore()
    partners = [to_rep, to_fy, to_tp] + [{"fz": at} for at in (near, far, across)]
    for partner in partners:
        pl.semaphore_signal(barrier, inc=1, device_id=partner, device_id_type=MESH)
    pl.semaphore_wait(barrier, len(partners))

    def slot(key):
        if key not in slots:
            slots[key] = len(slots)
            assert len(slots) <= RECEIVES
        return recv_sem.at[slots[key]]

    def push(key, src, device, dst=None, when=None):
        place = send_sem.at[len(sent)]
        arrive = slot(key)

        def copy():
            return pltpu.make_async_remote_copy(
                src_ref=src,
                dst_ref=src if dst is None else dst,
                send_sem=place,
                recv_sem=arrive,
                device_id=device,
                device_id_type=MESH,
            )

        sent.append((copy, when))
        assert len(sent) <= SENDS
        if when is None:
            copy().start()
        else:
            pl.when(when)(lambda: copy().start())

    def recv(key, ref, when=None):
        arrive = slot(key)

        def wait():
            pltpu.make_async_remote_copy(
                src_ref=ref,
                dst_ref=ref,
                send_sem=send_sem.at[0],
                recv_sem=arrive,
                device_id=to_tp,
                device_id_type=MESH,
            ).wait_recv()

        if when is None:
            wait()
        else:
            pl.when(when)(wait)

    def local(index, pairs):
        for src, dst in pairs:
            pltpu.make_async_copy(src, dst, local_sem.at[index]).start()

    def local_wait(index, ref):
        pltpu.make_async_copy(ref, ref, local_sem.at[index]).wait()

    def block(index, which, size):
        return pl.ds(pl.multiple_of((zs[index] * 2 + which) * size, size), size)

    def front_half(index, which, side):
        return front.at[side, :, block(index, which, rows), :]

    def front_block(index, which):
        return front.at[:, :, block(index, which, rows), :]

    back_side = pl.ds(pl.multiple_of(rep * (chans // 2), chans // 2), chans // 2)
    back_far = pl.ds(pl.multiple_of((1 - rep) * (chans // 2), chans // 2), chans // 2)

    def back_half(index, which, side):
        return back.at[side, block(index, which, back_cols)]

    def back_block(index, which):
        return back.at[:, block(index, which, back_cols)]

    step = half // STAGES
    up_rows = width // 2
    given = pl.ds(pl.multiple_of(rep * own_ff, own_ff), own_ff)
    taken = pl.ds(pl.multiple_of(2 * own_ff + rep * own_ff, own_ff), own_ff)
    turned = pl.ds(pl.multiple_of(3 * own_ff - rep * own_ff, own_ff), own_ff)

    def up_piece(part, units):
        return up.at[part * up_rows : (part + 1) * up_rows, units]

    def down_piece(part, units):
        return down.at[:, units, cuts[part] : cuts[part + 1]]

    cuts = [at * step for at in range(STAGES)] + [half - step // 2, half]
    stages = len(cuts) - 1
    early = 4
    flow = [("up", part, up_piece) for part in range(2)]
    flow += [("down", part, down_piece) for part in range(stages)]

    def cross_send(at, when=None):
        name, part, piece = flow[at]
        push((name, part, "z"), piece(part, given), {"fz": across}, piece(part, taken), when=when)

    def cross_turn(at, when):
        name, part, piece = flow[at]
        recv((name, part, "z"), piece(part, taken), when=when)
        push((name, part, "x"), piece(part, taken), to_rep, when=when)

    def cross_last(at):
        name, part, piece = flow[at]
        recv((name, part, "x"), piece(part, turned))

    def line_send(key, piece):
        push((key, 2), piece(0), {"fz": far}, when=middle)
        push((key, 3), piece(0), {"fz": far}, when=ends)
        push((key, 2), piece(0), {"fz": across}, when=middle)
        push((key, 1), piece(0), {"fz": near})

    def line_relay(key, piece):
        recv((key, 3), piece(3), when=middle)
        push((key, 3), piece(3), {"fz": near}, when=middle)

    def line_last(key, piece):
        recv((key, 3), piece(3), when=ends)

    local(0, [(hidden_hbm, stream.at[:, own_lanes])])
    push("hid", hidden_hbm, to_tp, stream.at[:, own_lanes])
    mine = block(0, fy, rows)
    local(
        1,
        [
            (hbm.at[:, side * cols : (side + 1) * cols], front.at[side, kind, mine, :])
            for side in range(2)
            for kind, hbm in enumerate((value_hbm, gate_hbm))
        ],
    )
    local(2, [(back_hbm, back_block(0, fy))])
    own_units = pl.ds(0, 2 * own_ff)
    local(3, [(up_hbm, up.at[:, own_units])])
    local(
        4,
        [
            (down_hbm.at[:, side * half : (side + 1) * half], down.at[side, own_units, :])
            for side in range(2)
        ],
    )

    local_wait(1, front_block(0, fy))
    line_send("zf", lambda index: front_half(index, fy, rep))
    push(("yf", 0, 0), front_half(0, fy, 0), to_fy)
    push(("yf", 0, 1), front_half(0, fy, 1), to_fy, when=middle)
    local_wait(2, back_block(0, fy))
    line_send("zb", lambda index: back_half(index, fy, back_side))

    halo[:, :HALO, :] = jnp.zeros((halo.shape[0], HALO, halo.shape[2]), f32)
    local_wait(0, stream.at[:, own_lanes])
    recv("hid", stream.at[:, pl.ds(pl.multiple_of((1 - tp) * half, half), half)])

    def norm_rows(at, carry):
        place = pl.ds(pl.multiple_of(at * 32, 32), 32)
        values = stream[place, :].astype(f32)
        scale = lax.rsqrt(jnp.sum(values * values, axis=-1, keepdims=True) / width + 1e-06)
        feat[0, place, :] = (values * scale * mix_gain[...]).astype(bf16)
        return carry

    lax.fori_loop(0, tokens // 32, norm_rows, 0)

    def front_on(index, when=None):
        push(("yf", index), front_half(index, fy, rep), to_fy, when=when)
        push(("xf", 0, index), front_half(index, fy, rep), to_rep, when=when)

    def front_turn(index, when=None):
        recv(("yf", index), front_half(index, 1 - fy, rep), when=when)
        push(("xf", 1, index), front_half(index, 1 - fy, rep), to_rep, when=when)

    def back_on(index):
        push(("yb", index), back_half(index, fy, back_side), to_fy)
        push(("xb", 0, index), back_half(index, fy, back_side), to_rep)

    def back_turn(index):
        recv(("yb", index), back_half(index, 1 - fy, back_side))
        push(("xb", 1, index), back_half(index, 1 - fy, back_side), to_rep)

    def front_cross():
        recv(("xf", 0, 1), front_half(1, fy, 1 - rep))
        push(("yf", "x"), front.at[1 - rep, 0, block(1, fy, rows), :], to_fy)

    def back_cross():
        recv(("xb", 0, 1), back_half(1, fy, back_far))
        push(("yb", "x"), back_half(1, fy, back_far), to_fy)

    recv(("zf", 1), front_half(1, fy, rep))
    front_on(1)
    line_relay("zf", lambda index: front_half(index, fy, rep))
    front_on(3, middle)
    recv(("zf", 2), front_half(2, fy, rep))
    front_on(2)
    recv(("yf", 1), front_half(1, 1 - fy, rep))
    push(("xf", "y"), front.at[rep, 1, block(1, 1 - fy, rows), :], to_rep)
    local_wait(3, up.at[:, own_units])
    local_wait(4, down.at[:, own_units, :])
    line_last("zf", lambda index: front_half(index, fy, rep))
    front_on(3, ends)
    front_cross()
    push(("yf", 0, 1), front_half(0, fy, 1), to_fy, when=ends)
    line_relay("zb", lambda index: back_half(index, fy, back_side))
    front_turn(3, middle)
    front_turn(2)
    front_turn(3, ends)
    recv(("zb", 1), back_half(1, fy, back_side))
    back_on(1)
    recv(("zb", 2), back_half(2, fy, back_side))
    back_on(2)
    line_last("zb", lambda index: back_half(index, fy, back_side))
    back_on(3)
    pl.semaphore_signal(pair_sem, inc=1, device_id=to_tp, device_id_type=MESH)
    push(("yb", 0), back_block(0, fy), to_fy)
    pl.semaphore_wait(pair_sem, 1)
    for at in range(len(flow)):
        cross_send(at, None if at < early else middle)

    recv(("yf", 0, 0), front_half(0, 1 - fy, 0))
    recv(("yf", 0, 1), front_half(0, 1 - fy, 1))
    recv(("xf", 0, 2), front_half(2, fy, 1 - rep))
    recv(("xf", 1, 2), front_half(2, 1 - fy, 1 - rep))
    recv(("yf", "x"), front.at[1 - rep, 0, block(1, 1 - fy, rows), :])
    recv(("xf", "y"), front.at[1 - rep, 1, block(1, 1 - fy, rows), :])
    recv(("xf", 0, 3), front_half(3, fy, 1 - rep))
    recv(("xf", 1, 3), front_half(3, 1 - fy, 1 - rep))

    sequences = tokens // LEN
    for side in range(2):
        value = jnp.dot(feat[0], front[side, 0], preferred_element_type=f32)
        gate = jnp.dot(feat[0], front[side, 1], preferred_element_type=f32)
        gated = value * jax.nn.sigmoid(gate)
        halo[:, HALO:, side * cols : (side + 1) * cols] = gated.reshape(sequences, LEN, cols)

    def filter_sequence(at, carry):
        place = pl.ds(pl.multiple_of(at * LEN, LEN), LEN)
        total = jnp.zeros((LEN, LANES), f32)
        squares = jnp.zeros((LEN, LANES), f32)
        for lane in range(chans // LANES):
            lanes = slice(lane * LANES, (lane + 1) * LANES)
            result = jnp.zeros((LEN, LANES), f32) + bias[:, lanes]
            for shift in range(SUBLANES):
                size = LEN + SUBLANES if shift else LEN
                part = None
                for start in range(0, HALO + 1, SUBLANES):
                    tap = start + shift - (HALO - KW + 1)
                    if 0 <= tap < KW:
                        term = taps[tap : tap + 1, lanes] * halo[at, start : start + size, lanes]
                        part = term if part is None else part + term
                if shift:
                    part = pltpu.roll(part, size - shift, 0)[:LEN]
                result = result + part
            filtered[place, lanes] = result
            total = total + result
            squares = squares + result * result
        stats[0, place, :] = total
        stats[1, place, :] = squares
        return carry

    middle_sequence = sequences - sequences // 2
    lax.fori_loop(0, middle_sequence, filter_sequence, 0)
    recv(("yb", 1), back_half(1, 1 - fy, back_side))
    back_cross()
    back_turn(2)
    lax.fori_loop(middle_sequence, sequences, filter_sequence, 0)
    back_turn(3)
    push("stats", stats, to_tp, stats_in)
    recv("stats", stats_in)

    def act_rows(at, carry):
        place = pl.ds(pl.multiple_of(at * 32, 32), 32)
        count = 2 * chans
        mean = jnp.sum(stats[0, place, :] + stats_in[0, place, :], axis=-1, keepdims=True) / count
        second_moment = (
            jnp.sum(stats[1, place, :] + stats_in[1, place, :], axis=-1, keepdims=True) / count
        )
        scale = lax.rsqrt(second_moment - mean * mean + 1e-05)
        centred = (filtered[place, :] - mean) * scale * chan_gain[...] + chan_bias[...]
        act[place, :] = (centred * jax.nn.sigmoid(centred)).astype(bf16)
        return carry

    lax.fori_loop(0, tokens // 32, act_rows, 0)

    recv(("yb", 0), back_block(0, 1 - fy))
    recv(("yb", "x"), back_half(1, 1 - fy, back_far))
    for index in range(2, LINE):
        recv(("xb", 0, index), back_half(index, fy, back_far))
        recv(("xb", 1, index), back_half(index, 1 - fy, back_far))

    def back_lanes(side, part):
        return pl.ds(pl.multiple_of(side * half + part * step, step), step)

    for part in range(STAGES):
        lanes = slice(part * step, (part + 1) * step)
        product = jnp.dot(act[...], back[:, back_lanes(1 - tp, part)], preferred_element_type=f32)
        mix_out[:, lanes] = product.astype(bf16)
    push("mix", mix_out, to_tp, mix_in)
    for part in range(STAGES):
        kept[part] = jnp.dot(act[...], back[:, back_lanes(tp, part)], preferred_element_type=f32)
    recv("mix", mix_in)

    def second_rows(at, carry):
        place = pl.ds(pl.multiple_of(at * 32, 32), 32)
        squares = jnp.zeros((32, LANES), f32)
        for part in range(STAGES):
            lanes = slice(part * step, (part + 1) * step)
            source = pl.ds(pl.multiple_of(tp * half + part * step, step), step)
            mixed = kept[part, place, :] + mix_in[place, lanes].astype(f32)
            value = (stream[place, source].astype(f32) + mixed).astype(bf16)
            second[place, lanes] = value
            value = value.astype(f32)
            value = value * value
            for lane in range(step // LANES):
                squares = squares + value[:, lane * LANES : (lane + 1) * LANES]
        square[place, :] = squares
        return carry

    lax.fori_loop(0, tokens // 32, second_rows, 0)
    push("square", square, to_tp, square_in)
    recv("square", square_in)

    def feed_rows(at, carry):
        place = pl.ds(pl.multiple_of(at * 32, 32), 32)
        mean = jnp.sum(square[place, :] + square_in[place, :], axis=-1, keepdims=True) / width
        scale = lax.rsqrt(mean + 1e-06)
        values = second[place, :].astype(f32) * scale * feed_gain[:, own_lanes]
        feat[0, place, own_lanes] = values.astype(bf16)
        return carry

    part_rows = tokens // 2

    bounds = {index: (0, part_rows, tokens) for index in range(3)}
    bounds[3] = (0, part_rows, part_rows + part_rows // 2, tokens)

    def feat_part(index, part, lanes, like=None):
        edges = bounds[index if like is None else like]
        return feat.at[index, edges[part] : edges[part + 1], lanes]

    other_lanes = pl.ds(pl.multiple_of((1 - tp) * half, half), half)

    def share(index, part):
        push(("pair", index, part), feat_part(index, part, own_lanes), to_tp)

    def shared(index, part):
        recv(("pair", index, part), feat_part(index, part, other_lanes))

    for part in range(2):
        lax.fori_loop(part * part_rows // 32, (part + 1) * part_rows // 32, feed_rows, 0)
        push(("line", part), feat_part(0, part, own_lanes), to_line, feat_part(1, part, own_lanes))
        push(("fy", part), feat_part(0, part, own_lanes), to_fy, feat_part(2, part, own_lanes))
        share(0, part)

    def up_slot(index, side, part=None):
        first, last = (0, tokens) if part is None else bounds[index][part : part + 2]
        for piece in range(2):
            lanes = slice((2 * side + piece) * own_ff, (2 * side + piece + 1) * own_ff)
            product = jnp.dot(
                feat[index, first:last, :], up[:, lanes], preferred_element_type=f32
            )
            product = jnp.square(jnp.maximum(product, 0.0))
            hidden[index, first:last, lanes] = product.astype(bf16)

    for at in range(early - 1):
        cross_turn(at, ends)
    shared(0, 0)
    shared(0, 1)
    up_slot(0, 0)
    cross_turn(0, middle)
    recv(("line", 0), feat_part(1, 0, own_lanes))
    push(("diag", 0), feat_part(1, 0, own_lanes), to_fy, feat_part(3, 0, own_lanes))
    share(1, 0)
    recv(("fy", 0), feat_part(2, 0, own_lanes))
    share(2, 0)
    cross_turn(1, middle)
    cross_turn(early - 1, ends)
    recv(("line", 1), feat_part(1, 1, own_lanes))
    share(1, 1)
    recv(("fy", 1), feat_part(2, 1, own_lanes))
    for part in (1, 2):
        push(
            ("diag", part),
            feat_part(2, part, own_lanes, 3),
            to_line,
            feat_part(3, part, own_lanes),
        )
    for at in range(early, len(flow)):
        cross_send(at, ends)
    share(2, 1)
    shared(1, 0)
    shared(1, 1)
    up_slot(1, 0)
    shared(2, 0)
    shared(2, 1)
    up_slot(2, 0)
    cross_turn(2, middle)
    cross_last(0)
    cross_last(1)
    up_slot(0, 1)
    recv(("diag", 0), feat_part(3, 0, own_lanes))
    share(3, 0)
    up_slot(1, 1)
    cross_turn(3, middle)
    up_slot(2, 1)
    shared(3, 0)
    for side in range(2):
        up_slot(3, side, 0)
    for part in (1, 2):
        recv(("diag", part), feat_part(3, part, own_lanes))
        share(3, part)
    for part in (1, 2):
        shared(3, part)
        for side in range(2):
            up_slot(3, side, part)

    turn_rows = tokens * 3 // 10

    def home(stage, index):
        return index if index or stage % 2 == 0 else STAGES

    def span(stage):
        return slice(cuts[stage], cuts[stage + 1])

    def products(stage, index):
        lanes = span(stage)
        product = jnp.dot(hidden[index], down[1 - tp, :, lanes], preferred_element_type=f32)
        pair_out[index, :, lanes] = product.astype(bf16)
        push(
            ("sum", index, stage),
            pair_out.at[index, :, lanes],
            to_tp,
            pair_in.at[index, :, lanes],
        )
        product = jnp.dot(hidden[index], down[tp, :, lanes], preferred_element_type=f32)
        kept[home(stage, index), :, : cuts[stage + 1] - cuts[stage]] = product

    def paired(stage, index, first, last):
        lanes = span(stage)
        own = kept[home(stage, index), first:last, : cuts[stage + 1] - cuts[stage]]
        return own + pair_in[index, first:last, lanes].astype(f32)

    def finish(stage):
        lanes = span(stage)
        recv(("sum", 0, stage), pair_in.at[0, :, lanes])
        recv(("near", 0, stage), rep_in.at[:, lanes])
        recv(("near", 1, stage), fy_in.at[:, lanes])
        feed = paired(stage, 0, 0, tokens)
        feed = feed + rep_in[:, lanes].astype(f32) + fy_in[:, lanes].astype(f32)
        result[:, lanes] = (second[:, lanes].astype(f32) + feed).astype(bf16)
        local(5 + stage, [(result.at[:, lanes], out.at[:, lanes])])

    def send_far(stage):
        lanes = span(stage)
        recv(("sum", 3, stage), pair_in.at[3, :, lanes])
        plane_out[2, :, lanes] = paired(stage, 3, 0, tokens).astype(bf16)
        for part, (rows_of, device) in enumerate(
            ((slice(0, turn_rows), to_line), (slice(turn_rows, tokens), to_fy))
        ):
            push(
                ("far", part, stage),
                plane_out.at[2, rows_of, lanes],
                device,
                diag_in.at[rows_of, lanes],
            )

    def send_near(stage):
        lanes = span(stage)
        recv(("sum", 1, stage), pair_in.at[1, :, lanes])
        plane_out[0, :turn_rows, lanes] = paired(stage, 1, 0, turn_rows).astype(bf16)
        recv(("far", 1, stage), diag_in.at[turn_rows:, lanes])
        plane_out[0, turn_rows:, lanes] = (
            paired(stage, 1, turn_rows, tokens) + diag_in[turn_rows:, lanes].astype(f32)
        ).astype(bf16)
        push(("near", 0, stage), plane_out.at[0, :, lanes], to_line, rep_in.at[:, lanes])
        recv(("sum", 2, stage), pair_in.at[2, :, lanes])
        plane_out[1, turn_rows:, lanes] = paired(stage, 2, turn_rows, tokens).astype(bf16)
        recv(("far", 0, stage), diag_in.at[:turn_rows, lanes])
        plane_out[1, :turn_rows, lanes] = (
            paired(stage, 2, 0, turn_rows) + diag_in[:turn_rows, lanes].astype(f32)
        ).astype(bf16)
        push(("near", 1, stage), plane_out.at[1, :, lanes], to_fy, fy_in.at[:, lanes])

    cross_last(2)
    products(0, 3)
    products(0, 1)
    send_far(0)
    for stage in range(stages):
        last = stage + 1 == stages
        if not last:
            if stage == 0:
                cross_turn(early, None)
            cross_last(stage + 3)
            products(stage + 1, 3)
        products(stage, 2)
        products(stage, 0)
        if not last:
            send_far(stage + 1)
        send_near(stage)
        if early + stage + 1 < len(flow):
            cross_turn(early + stage + 1, None)
        if not last:
            products(stage + 1, 1)
        if stage:
            finish(stage - 1)
    finish(stages - 1)
    for stage in range(stages):
        lanes = span(stage)
        pltpu.make_async_copy(result.at[:, lanes], out.at[:, lanes], local_sem.at[5 + stage]).wait()

    for copy, when in sent:
        if when is None:
            copy().wait_send()
        else:
            pl.when(when)(lambda copy=copy: copy().wait_send())


def fused(*arrays):
    hidden_in, mix_gain, w_value, w_gate, taps, bias, gain, shift, w_back, feed_gain, w_up, w_down = arrays
    tokens, half = hidden_in.shape
    _, chans = w_value.shape
    width, ff = 2 * half, w_up.shape[1] // 2 * LINE
    bf16, f32 = jnp.bfloat16, jnp.float32
    vmem, hbm = pl.BlockSpec(memory_space=pltpu.VMEM), pl.BlockSpec(memory_space=pltpu.HBM)
    step = half // STAGES
    scratch = [
        ((tokens, width), bf16),
        ((4, tokens, width), bf16),
        ((2, 2, width, chans // 2), bf16),
        ((chans, width), bf16),
        ((tokens // LEN, HALO + LEN, chans), f32),
        ((tokens, chans), f32),
        ((tokens, chans), bf16),
        ((2, tokens, LANES), f32),
        ((2, tokens, LANES), f32),
        ((tokens, half), bf16),
        ((tokens, half), bf16),
        ((STAGES + 1, tokens, step), f32),
        ((tokens, half), bf16),
        ((tokens, LANES), f32),
        ((tokens, LANES), f32),
        ((width, ff), bf16),
        ((2, ff, half), bf16),
        ((4, tokens, ff), bf16),
        ((4, tokens, half), bf16),
        ((4, tokens, half), bf16),
        ((3, tokens, half), bf16),
        ((tokens, half), bf16),
        ((tokens, half), bf16),
        ((tokens, half), bf16),
    ]
    return pl.pallas_call(
        fused_kernel,
        out_shape=jax.ShapeDtypeStruct((tokens, half), bf16),
        in_specs=[hbm, vmem, hbm, hbm, vmem, vmem, vmem, vmem, hbm, vmem, hbm, hbm],
        out_specs=hbm,
        scratch_shapes=[pltpu.VMEM(shape, kind) for shape, kind in scratch]
        + [
            pltpu.SemaphoreType.DMA((6 + STAGES,)),
            pltpu.SemaphoreType.DMA((SENDS,)),
            pltpu.SemaphoreType.DMA((RECEIVES,)),
            pltpu.SemaphoreType.REGULAR,
        ],
        compiler_params=pltpu.CompilerParams(
            collective_id=0, has_side_effects=True, vmem_limit_bytes=67043328
        ),
    )(
        hidden_in,
        mix_gain[None],
        w_value,
        w_gate,
        taps,
        bias[None],
        gain[None],
        shift[None],
        w_back,
        feed_gain[None],
        w_up,
        w_down,
    )


def fits(mesh):
    return mesh.shape["rep"] == 2 and mesh.shape["fs"] == 2 * LINE and mesh.shape["tp"] == 2


def solution(mesh):
    n_rep, n_fs, n_tp = mesh.shape["rep"], mesh.shape["fs"], mesh.shape["tp"]
    split = Mesh(mesh.devices.reshape(n_rep, n_fs // 2, 2, n_tp), ("rep", "fz", "fy", "tp"))
    fs = ("fz", "fy")
    rows = P(("rep", "fz", "fy"), "tp")
    placed = (
        rows,
        P(),
        P(fs, "tp"),
        P(fs, "tp"),
        P(None, "tp"),
        P("tp"),
        P("tp"),
        P("tp"),
        P("tp", fs),
        P(),
        P(None, ("fz", "fy", "tp")),
        P(("fz", "fy", "tp"), None),
    )
    if fits(mesh):
        return jax.shard_map(fused, mesh=split, in_specs=placed, out_specs=rows, check_vma=False)
    return jax.shard_map(block, mesh=split, in_specs=placed, out_specs=rows, check_vma=False)
```
